256 devices in a mesh: sp: 16 (over y, x), tp: 16 (over z, core).
Axes of the slice: x: 4, y: 4, z: 8, core: 2. Of those that a mesh axis runs over, the one named last changes fastest.
Arguments:
- latent: bfloat16 [8192, 4096], P(('sp', 'tp')), may hold values from -6 to 6
- context: bfloat16 [512, 4096], P('sp'), may hold values from -6 to 6
- condition: float32 [4096], replicated, may hold values from -6 to 6
- context_condition: float32 [4096], replicated, may hold values from -6 to 6
- modulation: bfloat16 [3, 4096, 4096], P(None, 'sp', 'tp'), may hold values from -0.09375 to 0.09375
- query_weight: bfloat16 [4096, 4096], P(None, 'tp'), as said below
- key_weight: bfloat16 [4096, 4096], P(None, 'tp'), as said below
- value_weight: bfloat16 [4096, 4096], P(None, 'tp'), may hold values from -0.09375 to 0.09375
- lambdas: float32 [16], P('tp'), may hold values from 0.3 to 0.8
- context_lift: float32 [16], P('tp'), may hold values from 1.5 to 3
- head_gain: float32 [256], replicated, may hold values from 0.1 to 1.9
- output_weight: bfloat16 [4096, 4096], P('tp'), may hold values from -0.09375 to 0.09375
Outputs:
- result: bfloat16 [8192, 4096], P(('sp', 'tp'))
The draws below stay inside these ranges and needn't reach their ends.
Inputs may be any that keep to these rules, and one draw needn't show every extreme that they name: `query_weight`: entries lie within 200 / sqrt(4096) in magnitude. `key_weight`: entries lie within 6 / sqrt(4096) in magnitude.
All inputs are finite; a program needn't handle non-finite values.
Results may differ from the reference program's by a relative error of at most 0.025.
Values may be sent and summed in bfloat16 or wider, within the bound.
No kernel may reach another device: no remote copies, remote signals or barrier semaphores. Data moves between devices by JAX's collectives and lax.ppermute only.
A program may use at most 64 MiB of HBM per device.

```python
import math
import jax
import jax.numpy as jnp
from jax import lax

D = 4096
HEADS = 16
HEAD_DIM = 256
GRID_W = 64
CTX = 512
SEQ = 8192


def common_keys(key):
    gaussian = jax.random.normal(jax.random.fold_in(key, 101), (D, HEADS * HEAD_DIM), jnp.float32)
    return jnp.clip(gaussian, -6.0, 6.0) * D ** (-0.5)


def draw_key_weight(key, part):
    return common_keys(key).astype(jnp.bfloat16)


def draw_query_weight(key, part):
    gaussian = jax.random.normal(jax.random.fold_in(key, 202), (D, HEADS * HEAD_DIM), jnp.float32)
    independent = jnp.clip(gaussian, -6.0, 6.0) * D ** (-0.5)
    return independent.astype(jnp.bfloat16)


def steps_of(rng, extent, shards, low, high):
    gain, own = 1.0, jax.random.fold_in(rng, 6)
    for dim, shards_of in shards:
        heights = jnp.exp(jax.random.uniform(jax.random.fold_in(own, dim), (shards_of,), jnp.float32, low / len(shards), high / len(shards)))
        gain = gain * jnp.repeat(heights, extent[dim] // shards_of).reshape([-1 if axis == dim else 1 for axis in range(len(extent))])
    return gain


def scatter_about(own_key, extent, scale, reach, cuts=(), kind=jnp.bfloat16):
    factor_of = steps_of(own_key, extent, cuts, -0.22, 0.18) if cuts else 1.0
    values = jax.random.normal(own_key, extent, jnp.float32) * scale * factor_of
    return jnp.minimum(jnp.maximum(values, -reach), reach).astype(kind)


def setup_inputs(seed: int = 0) -> dict:
    keys = jax.random.split(jax.random.key(seed), 13)
    latent = scatter_about(keys[0], (SEQ, D), 1.0, 6.0, ((0, 256),))
    context = scatter_about(keys[1], (CTX, D), 1.0, 6.0, ((0, 16),))
    condition = scatter_about(keys[2], (D,), 1.0, 6.0, (), jnp.float32)
    context_condition = scatter_about(keys[3], (D,), 1.0, 6.0, (), jnp.float32)
    modulation = scatter_about(keys[4], (3, D, D), D ** -0.5, 0.09375, ((1, 16), (2, 16)))
    query_weight = draw_query_weight(jax.random.fold_in(keys[12], 71), 0)
    key_weight = draw_key_weight(jax.random.fold_in(keys[12], 71), 0)
    value_weight = scatter_about(keys[7], (D, HEADS * HEAD_DIM), D ** -0.5, 0.09375, ((1, 16),))
    lambdas = jnp.clip(0.3 + 0.5 * jax.random.uniform(keys[8], (HEADS,), jnp.float32) ** steps_of(keys[8], (HEADS,), ((0, 16),), -0.2, 0.2), 0.3, 0.8)
    context_lift = jnp.clip(1.5 + 1.5 * jax.random.uniform(keys[9], (HEADS,), jnp.float32) ** steps_of(keys[9], (HEADS,), ((0, 16),), -0.2, 0.2), 1.5, 3.0)
    head_gain = jnp.clip(1.0 + 0.18 * jax.random.normal(keys[10], (HEAD_DIM,), jnp.float32), 0.1, 1.9)
    output_weight = scatter_about(keys[11], (HEADS * HEAD_DIM, D), (HEADS * HEAD_DIM) ** -0.5, 0.09375, ((0, 16),))
    return {"latent": latent, "context": context, "condition": condition, "context_condition": context_condition, "modulation": modulation, "query_weight": query_weight, "key_weight": key_weight, "value_weight": value_weight, "lambdas": lambdas, "context_lift": context_lift, "head_gain": head_gain, "output_weight": output_weight}


ROPE_BASE = 10000.0
EPSILON = 1e-05

def modulate(tokens_in, offset, scaling):
    values = tokens_in.astype(jnp.float32)
    center = lax.optimization_barrier(jnp.mean(values, axis=-1, keepdims=True))
    spread = lax.optimization_barrier(jnp.mean(jnp.square(values - center), axis=-1, keepdims=True))
    normed = (values - center) * lax.rsqrt(spread + EPSILON)
    return (normed * (1.0 + scaling) + offset).astype(jnp.bfloat16)

def rotate(tensor, places):
    number, head_count, head_width = tensor.shape
    quarter = head_width // 4
    eighth = head_width // 8
    inverse = ROPE_BASE ** (-jnp.arange(eighth, dtype=jnp.float32) / eighth)
    grid_row = (places // GRID_W).astype(jnp.float32)
    grid_col = (places % GRID_W).astype(jnp.float32)
    angles = jnp.stack([grid_row[:, None] * inverse, grid_col[:, None] * inverse], axis=1)
    cosine = jnp.cos(angles)[:, None, None, :, :]
    sine_table = jnp.sin(angles)[:, None, None, :, :]
    pieces = tensor.reshape(number, head_count, 2, 2, quarter)
    first_half = pieces[..., :eighth]
    second = pieces[..., eighth:]
    turned = jnp.concatenate([first_half * cosine - second * sine_table, second * cosine + first_half * sine_table], axis=-1)
    return turned.reshape(number, head_count, head_width)

def reference(latent, context, condition, context_condition, modulation, query_weight, key_weight, value_weight, lambdas, context_lift, head_gain, output_weight):
    silu_pair = jax.nn.silu(jnp.stack([condition, context_condition])).astype(jnp.bfloat16)
    mod_vectors = jnp.einsum('cd,rde->cre', silu_pair.astype(jnp.float32), modulation.astype(jnp.float32))
    normed = modulate(latent, mod_vectors[0, 0], mod_vectors[0, 1])
    normed_context = modulate(context, mod_vectors[1, 0], mod_vectors[1, 1])
    seq_len = latent.shape[0]
    half_width = HEAD_DIM // 2
    scale_factor = half_width ** (-0.5)
    query_raw = jnp.dot(normed, query_weight, preferred_element_type=jnp.float32).astype(jnp.bfloat16)
    key_raw = jnp.dot(normed, key_weight, preferred_element_type=jnp.float32).astype(jnp.bfloat16)
    latent_values = jnp.dot(normed, value_weight, preferred_element_type=jnp.float32).astype(jnp.bfloat16)
    context_keys = jnp.dot(normed_context, key_weight, preferred_element_type=jnp.float32).astype(jnp.bfloat16)
    context_values = jnp.dot(normed_context, value_weight, preferred_element_type=jnp.float32).astype(jnp.bfloat16)
    places = jnp.arange(seq_len, dtype=jnp.int32)
    queries = rotate(query_raw.astype(jnp.float32).reshape(seq_len, HEADS, HEAD_DIM), places).astype(jnp.bfloat16)
    latent_keys = rotate(key_raw.astype(jnp.float32).reshape(seq_len, HEADS, HEAD_DIM), places).astype(jnp.bfloat16)
    all_keys = jnp.concatenate([context_keys.reshape(CTX, HEADS, HEAD_DIM), latent_keys], axis=0)
    all_values = jnp.concatenate([context_values.reshape(CTX, HEADS, HEAD_DIM), latent_values.reshape(seq_len, HEADS, HEAD_DIM)], axis=0)
    key_total = CTX + seq_len
    block_len = math.gcd(seq_len, 1024)

    def one_head(inputs):
        head_queries, head_keys, head_values, head_lambda, head_lift = inputs
        lift_row = jnp.where(jnp.arange(key_total) < CTX, head_lift, 0.0)

        def one_block(block_queries):
            outputs = []
            for map_index in range(2):
                low_col = map_index * half_width
                scores = jnp.dot(block_queries[:, low_col:low_col + half_width], head_keys[:, low_col:low_col + half_width].T, preferred_element_type=jnp.float32) * scale_factor + lift_row
                row_peak = lax.optimization_barrier(jnp.max(scores, axis=1, keepdims=True))
                weights = jnp.exp(scores - row_peak)
                row_sums = lax.optimization_barrier(jnp.sum(weights, axis=1, keepdims=True))
                outputs.append(jnp.dot(weights.astype(jnp.bfloat16), head_values, preferred_element_type=jnp.float32) / row_sums)
            difference = outputs[0] - head_lambda * outputs[1]
            scaled = difference * lax.rsqrt(lax.optimization_barrier(jnp.mean(jnp.square(difference), axis=1, keepdims=True)) + EPSILON) * head_gain
            return scaled.astype(jnp.bfloat16)
        blocks = head_queries.reshape(seq_len // block_len, block_len, HEAD_DIM)
        return lax.map(one_block, blocks).reshape(seq_len, HEAD_DIM)
    heads_out = lax.map(one_head, (queries.transpose(1, 0, 2), all_keys.transpose(1, 0, 2), all_values.transpose(1, 0, 2), lambdas, context_lift))
    attended = heads_out.transpose(1, 0, 2).reshape(seq_len, HEADS * HEAD_DIM)
    mixture = jnp.dot(attended, output_weight, preferred_element_type=jnp.float32)
    return (latent.astype(jnp.float32) + mod_vectors[0, 2] * mixture).astype(jnp.bfloat16)
```

```python
import functools
import math

import jax
import jax.numpy as jnp
from jax import lax
from jax.experimental import pallas as pl
from jax.experimental.pallas import tpu as pltpu
from jax.sharding import Mesh
from jax.sharding import PartitionSpec as P

GRID_W = 64
ROPE_BASE = 10000.0
EPSILON = 1e-05
LOG2E = math.log2(math.e)
SP = ("y", "x")
TP = ("z", "core")
ALL = SP + TP
F32 = jnp.float32
BF16 = jnp.bfloat16
ANY = pl.ANY


def hop(value, axis, step):
    size = lax.axis_size(axis)
    return lax.ppermute(value, axis, [(i, (i + step) % size) for i in range(size)])


def from_everyone(shard, axis):
    copies = jnp.broadcast_to(shard, (lax.axis_size(axis), *shard.shape))
    return lax.all_to_all(copies, axis, split_axis=0, concat_axis=0, tiled=True)


def modulation_vectors(condition, context_condition, modulation):
    rows_block = modulation.shape[1]
    silu_pair = jax.nn.silu(jnp.stack([condition, context_condition])).astype(BF16)
    own_rows = lax.dynamic_slice_in_dim(silu_pair, lax.axis_index(SP) * rows_block, rows_block, 1)
    partial_mod = jnp.einsum("cd,rde->cre", own_rows, modulation, preferred_element_type=F32)
    partial_mod = partial_mod.reshape(-1, partial_mod.shape[-1])[:5]
    summed = jnp.sum(from_everyone(partial_mod, SP), axis=0)
    gathered = from_everyone(summed, TP)
    return jnp.moveaxis(gathered, 0, 1).reshape(5, -1)


def rope_tables(rows_own, width):
    z_size = lax.axis_size("z")
    lane = jnp.arange(width)
    eighth = width // 8
    inverse = ROPE_BASE ** (-(lane % eighth).astype(F32) / eighth)
    row = lax.axis_index(SP) * z_size + (lax.axis_index("z") + jnp.arange(z_size)) % z_size
    col = lax.axis_index("core") * rows_own + jnp.arange(rows_own)
    angles = jnp.concatenate([row, col]).astype(F32)[:, None] * inverse
    by_row = (lane % (width // 2)) < width // 4

    def spread(table):
        full = jnp.where(by_row, table[:z_size, None, :], table[None, z_size:, :])
        return full.reshape(z_size * rows_own, width)

    return spread(jnp.cos(angles)), spread(jnp.sin(angles))


def swap_matrix(width):
    source = jnp.arange(width)[:, None]
    target = jnp.arange(width)[None, :]
    eighth = width // 8
    low = target % (2 * eighth) < eighth
    minus = (source == target + eighth) & low
    plus = (source == target - eighth) & ~low
    return plus.astype(BF16) - minus.astype(BF16)


def project(pieces, context_rows, vectors, weights, cosine, sine, swap):
    model = vectors.shape[1]
    width = weights[0].shape[1]
    lengths = [piece.shape[0] for piece in pieces] + [context_rows.shape[0]]
    rows = sum(lengths[:-1])
    total = sum(lengths)
    count = len(pieces) + 1
    step = 16

    def kernel(*refs):
        token_refs = refs[:count]
        vec, cos_ref, sin_ref, swap_ref = refs[count : count + 4]
        weight_refs = refs[count + 4 : count + 10]
        q_own, kv_own, q_far, kv_far = refs[count + 10 : count + 14]
        buffer, normed, raw, sems = refs[count + 14 :]
        for j in range(6):
            pltpu.make_async_copy(weight_refs[j], buffer.at[j], sems.at[j]).start()
        start = 0
        for index, ref in enumerate(token_refs):
            base = 3 if index == count - 1 else 0
            for low in range(0, lengths[index], step):
                values = ref[low : low + step, :].astype(F32)
                center = jnp.mean(values, axis=-1, keepdims=True)
                shifted = values - center
                spread = jnp.mean(shifted * shifted, axis=-1, keepdims=True)
                out = shifted * lax.rsqrt(spread + EPSILON)
                out = out * (1.0 + vec[base + 1 : base + 2, :]) + vec[base : base + 1, :]
                normed[start + low : start + low + step, :] = out.astype(BF16)
            start += lengths[index]

        def one(j, carry):
            pltpu.make_async_copy(weight_refs[0], buffer.at[j], sems.at[j]).wait()
            raw[j] = jnp.dot(normed[...], buffer[j], preferred_element_type=F32).astype(BF16)
            return carry

        lax.fori_loop(0, 6, one, 0)

        def turn(value):
            turned = jnp.dot(value, swap_ref[...], preferred_element_type=F32)
            return (value.astype(F32) * cos_ref[...] + turned * sin_ref[...]).astype(BF16)

        for base, q_ref, kv_ref in ((0, q_own, kv_own), (3, q_far, kv_far)):
            q_ref[...] = turn(raw[base, :rows, :])
            kv_ref[0, :rows, :] = turn(raw[base + 1, :rows, :])
            kv_ref[0, rows:, :] = raw[base + 1, rows:, :]
            kv_ref[1, :, :] = raw[base + 2]

    vmem = pl.BlockSpec(memory_space=pltpu.VMEM)
    shapes = [(rows, width), (2, total, width)] * 2
    return pl.pallas_call(
        kernel,
        out_shape=[jax.ShapeDtypeStruct(shape, BF16) for shape in shapes],
        in_specs=[vmem] * (count + 4) + [pl.BlockSpec(memory_space=ANY)] * 6,
        out_specs=[vmem] * 4,
        scratch_shapes=[
            pltpu.VMEM((6, model, width), BF16),
            pltpu.VMEM((total, model), BF16),
            pltpu.VMEM((6, total, width), BF16),
            pltpu.SemaphoreType.DMA((6,)),
        ],
        cost_estimate=pl.CostEstimate(
            flops=2 * 6 * total * model * width, bytes_accessed=12 * model * width, transcendentals=0
        ),
        name="project",
    )(*pieces, context_rows, vectors, cosine, sine, swap, *weights)


def attend(queries, arrays, units, lift, state=None, final=None):
    blocks, rows, width = queries.shape
    half = width // 2
    number = len(arrays)
    total = arrays[0].shape[-2]
    context = total - rows
    scale = half ** (-0.5) * LOG2E
    first, last = state is None, final is not None
    n = len(units)

    def kernel(*refs):
        lift_ref, q_ref = refs[:2]
        key_refs = refs[2 : 2 + number]
        rest = refs[2 + number :]
        if not first:
            m_in, l_in, o_in = rest[:3]
            rest = rest[3:]
        if last:
            lambda_ref, gain_ref, out_ref, scores, sums, accs = rest
        else:
            m_out, l_out, o_out, scores = rest
        lift_two = lift_ref[0] * LOG2E

        def part(place, low, high, left, right):
            ref = key_refs[place[0]]
            return ref[(*place[1:], slice(low, high), slice(left, right))]

        for m in range(2):
            left, right = m * half, (m + 1) * half
            q = q_ref[0, :, left:right]
            peak = None
            for u, (key_place, _) in enumerate(units):
                keys = part(key_place, 0, rows, left, right)
                block = lax.dot_general(q, keys, (((1,), (1,)), ((), ())), preferred_element_type=F32)
                scores[:, u * rows : (u + 1) * rows] = block
                for lane in range(0, rows, 128):
                    piece = block[:, lane : lane + 128]
                    peak = piece if peak is None else jnp.maximum(peak, piece)
            keys = jnp.concatenate([part(k, rows, total, left, right) for k, _ in units], axis=0)
            lifted = lax.dot_general(q, keys, (((1,), (1,)), ((), ())), preferred_element_type=F32)
            lifted = lifted * scale + lift_two
            top = jnp.maximum(
                jnp.max(peak, axis=1, keepdims=True) * scale, jnp.max(lifted, axis=1, keepdims=True)
            )
            if first:
                new = top
                total_sum = None
                out = None
            else:
                old = m_in[m, 0, :, :1]
                new = jnp.maximum(old, top)
                fading = jnp.exp2(old - new)
                total_sum = l_in[m, 0] * fading
                out = o_in[m, 0] * fading
            if last:
                acc_ref = accs.at[m]
            else:
                acc_ref = o_out.at[m, 0]
            values = jnp.concatenate([part(v, rows, total, 0, width) for _, v in units], axis=0)
            weights = jnp.exp2(lifted - new)
            extra = jnp.sum(weights, axis=1, keepdims=True)
            product = jnp.dot(weights.astype(BF16), values, preferred_element_type=F32)
            acc_ref[...] = product if out is None else out + product
            for u, (_, value_place) in enumerate(units):
                weights = jnp.exp2(scores[:, u * rows : (u + 1) * rows] * scale - new)
                for lane in range(0, rows, 128):
                    piece = weights[:, lane : lane + 128]
                    total_sum = piece if total_sum is None else total_sum + piece
                values = part(value_place, 0, rows, 0, width)
                acc_ref[...] += jnp.dot(weights.astype(BF16), values, preferred_element_type=F32)
            lanes = lax.broadcasted_iota(jnp.int32, total_sum.shape, 1)
            total_sum = total_sum + jnp.where(lanes == 0, extra, 0.0)
            if last:
                sums[m] = jnp.broadcast_to(jnp.sum(total_sum, axis=1, keepdims=True), total_sum.shape)
            else:
                l_out[m, 0] = total_sum
                m_out[m, 0] = jnp.broadcast_to(new, total_sum.shape)
        if last:
            difference = accs[0] / sums[0, :, :1] - lambda_ref[0] * (accs[1] / sums[1, :, :1])
            power = jnp.mean(difference * difference, axis=1, keepdims=True)
            out_ref[0] = (difference * lax.rsqrt(power + EPSILON) * gain_ref[...]).astype(BF16)

    smem = pl.BlockSpec(memory_space=pltpu.SMEM)

    def whole(array):
        return pl.BlockSpec(array.shape, lambda i, dims=array.ndim: (0,) * dims)

    by_query = pl.BlockSpec((1, rows, width), lambda i: (i, 0, 0))
    narrow = pl.BlockSpec((2, 1, rows, 128), lambda i: (0, i, 0, 0))
    wide = pl.BlockSpec((2, 1, rows, width), lambda i: (0, i, 0, 0))
    inputs = [lift, queries, *arrays]
    in_specs = [smem, by_query, *(whole(array) for array in arrays)]
    scratch = [pltpu.VMEM((rows, n * rows), F32)]
    if not first:
        inputs += list(state)
        in_specs += [narrow, narrow, wide]
    if last:
        lambdas, gain = final
        inputs += [lambdas, gain]
        in_specs += [smem, pl.BlockSpec(gain.shape, lambda i: (0, 0))]
        out_shape = jax.ShapeDtypeStruct((blocks, rows, width), BF16)
        out_specs = by_query
        scratch += [pltpu.VMEM((2, rows, 128), F32), pltpu.VMEM((2, rows, width), F32)]
    else:
        out_shape = [
            jax.ShapeDtypeStruct((2, blocks, rows, 128), F32),
            jax.ShapeDtypeStruct((2, blocks, rows, 128), F32),
            jax.ShapeDtypeStruct((2, blocks, rows, width), F32),
        ]
        out_specs = [narrow, narrow, wide]
    return pl.pallas_call(
        kernel,
        grid=(blocks,),
        out_shape=out_shape,
        in_specs=in_specs,
        out_specs=out_specs,
        scratch_shapes=scratch,
        cost_estimate=pl.CostEstimate(
            flops=2 * 6 * blocks * rows * n * total * half,
            bytes_accessed=4 * n * total * width,
            transcendentals=2 * blocks * rows * n * total,
        ),
        name="attend",
    )(*inputs)


def output_product(own, far, weight_own, weight_far):
    rows, width = own.shape
    model = weight_own.shape[1]
    block = 512

    def kernel(own_ref, far_ref, a_ref, b_ref, out_ref):
        product = jnp.dot(own_ref[...], a_ref[...], preferred_element_type=F32)
        product += jnp.dot(far_ref[...], b_ref[...], preferred_element_type=F32)
        out_ref[...] = product.astype(BF16)

    row_spec = pl.BlockSpec((rows, width), lambda i: (0, 0))
    weight_spec = pl.BlockSpec((width, block), lambda i: (0, i))
    return pl.pallas_call(
        kernel,
        grid=(model // block,),
        out_shape=jax.ShapeDtypeStruct((rows, model), BF16),
        in_specs=[row_spec, row_spec, weight_spec, weight_spec],
        out_specs=pl.BlockSpec((rows, block), lambda i: (0, i)),
        cost_estimate=pl.CostEstimate(
            flops=4 * rows * width * model, bytes_accessed=4 * width * model, transcendentals=0
        ),
        name="output_product",
    )(own, far, weight_own, weight_far)


def plus(first, second):
    return (first.astype(F32) + second.astype(F32)).astype(BF16)


def shards(
    latent,
    context,
    condition,
    context_condition,
    modulation,
    query_weight,
    key_weight,
    value_weight,
    lambdas,
    context_lift,
    head_gain,
    output_weight,
):
    up1, down1 = hop(latent, "z", 1), hop(latent, "z", -1)
    up2, down2 = hop(up1, "z", 1), hop(down1, "z", -1)
    up3, down3 = hop(up2, "z", 1), hop(down2, "z", -1)
    middle = latent.shape[0] // 2
    up4, down4 = hop(up3[:middle], "z", 1), hop(down3[middle:], "z", -1)
    pieces = [latent, down1, down2, down3, up4, down4, up3, up2, up1]

    own_weights = [query_weight, key_weight, value_weight]
    far_weights = [hop(weight, "core", 1) for weight in own_weights]
    far_output = hop(output_weight, "core", 1)

    vectors = modulation_vectors(condition, context_condition, modulation)
    cosine, sine = rope_tables(latent.shape[0], query_weight.shape[1])
    swap = swap_matrix(query_weight.shape[1])
    share = context.shape[0] // lax.axis_size("core")
    context_rows = lax.dynamic_slice_in_dim(context, lax.axis_index("core") * share, share, 0)

    q_a, kv_a, q_send, kv_send = project(
        pieces, context_rows, vectors, own_weights + far_weights, cosine, sine, swap
    )
    kv_b = hop(kv_send, "core", 1)
    q_b = hop(q_send, "core", 1)
    queries = jnp.stack([q_a, q_b])

    ax_p, ax_m = hop(kv_a, "x", 1), hop(kv_a, "x", -1)
    ay_p, ay_m = hop(kv_a, "y", 1), hop(kv_a, "y", -1)
    bx_p, bx_m = hop(kv_b, "x", 1), hop(kv_b, "x", -1)
    by_p, by_m = hop(kv_b, "y", 1), hop(kv_b, "y", -1)
    xp1 = hop(jnp.stack([ay_p, ay_m, ax_p]), "x", 1)
    xm1 = hop(jnp.stack([ay_p, ay_m, bx_m]), "x", -1)
    yp1 = hop(jnp.stack([bx_p, bx_m, ay_p]), "y", 1)
    ym1 = hop(jnp.stack([bx_p, bx_m, by_m]), "y", -1)
    xp2 = hop(jnp.stack([yp1[2], xp1[:2, 0]]), "x", 1)
    xm2 = hop(jnp.stack([yp1[2], xm1[:2, 1]]), "x", -1)
    yp2 = hop(jnp.stack([xm1[2], yp1[:2, 0]]), "y", 1)
    ym2 = hop(jnp.stack([xm1[2], ym1[:2, 1]]), "y", -1)
    xp3, xm3 = hop(xp2[0, 0], "x", 1), hop(xm2[0, 1], "x", -1)
    yp3, ym3 = hop(yp2[0, 0], "y", 1), hop(ym2[0, 1], "y", -1)

    def plain(number):
        return [((i, 0), (i, 1)) for i in range(number)]

    state = attend(queries, [kv_a, kv_b], plain(2), context_lift)
    state = attend(
        queries, [ax_p, ax_m, ay_p, ay_m, bx_p, bx_m, by_p, by_m], plain(8), context_lift, state
    )
    state = attend(
        queries,
        [xp1, xm1, yp1, ym1],
        [((i, j, 0), (i, j, 1)) for i in range(4) for j in range(3)],
        context_lift,
        state,
    )
    state = attend(
        queries,
        [xp2, xm2, yp2, ym2],
        [((i, 0, 0), (i, 0, 1)) for i in range(4)]
        + [((i, 1, j), (i + 1, 1, j)) for i in (0, 2) for j in range(2)],
        context_lift,
        state,
    )
    attended = attend(
        queries,
        [xp3, xm3, yp3, ym3],
        [((0,), (1,)), ((2,), (3,))],
        context_lift,
        state,
        (lambdas, head_gain[None]),
    )

    far_heads = hop(attended[1], "core", 1)
    product = output_product(attended[0], far_heads, output_weight, far_output)
    share = product.reshape(-1, *latent.shape)
    up = hop(share[4, :middle], "z", 1)
    down = hop(share[4, middle:], "z", -1)
    up = hop(jnp.concatenate([plus(share[3, :middle], up), share[3, middle:]]), "z", 1)
    down = hop(jnp.concatenate([share[5, :middle], plus(share[5, middle:], down)]), "z", -1)
    up, down = hop(plus(share[2], up), "z", 1), hop(plus(share[6], down), "z", -1)
    up, down = hop(plus(share[1], up), "z", 1), hop(plus(share[7], down), "z", -1)
    mixture = share[0].astype(F32) + up.astype(F32) + down.astype(F32)
    return (latent.astype(F32) + vectors[2] * mixture).astype(BF16)


def solution(mesh):
    split = Mesh(mesh.devices.reshape(4, 4, mesh.shape["tp"] // 2, 2), ALL)
    return jax.shard_map(
        shards,
        mesh=split,
        in_specs=(
            P(ALL, None),
            P(SP, None),
            P(),
            P(),
            P(None, SP, TP),
            P(None, TP),
            P(None, TP),
            P(None, TP),
            P(TP),
            P(TP),
            P(),
            P(TP, None),
        ),
        out_specs=P(ALL, None),
        check_vma=False,
    )
```

```python
import functools
import itertools
import math

import jax
import jax.numpy as jnp
from jax import lax
from jax.experimental import pallas as pl
from jax.experimental.pallas import tpu as pltpu
from jax.sharding import Mesh
from jax.sharding import PartitionSpec as P

GRID_W = 64
ROPE_BASE = 10000.0
EPSILON = 1e-05
LOG2E = math.log2(math.e)
SP = ("y", "x")
TP = ("z", "core")
ALL = SP + TP
F32 = jnp.float32
BF16 = jnp.bfloat16
ANY = pl.ANY


def hop(value, axis, step):
    size = lax.axis_size(axis)
    return lax.ppermute(value, axis, [(i, (i + step) % size) for i in range(size)])


def hop_by_core(value, axes, step):
    names = tuple(name for name in ALL if name in (*axes, "core"))
    sizes = [lax.axis_size(name) for name in names]
    pairs = []
    for place in itertools.product(*(range(size) for size in sizes)):
        target = list(place)
        at = names.index(axes[place[names.index("core")]])
        target[at] = (target[at] + step) % sizes[at]
        flat = [0, 0]
        for k, where in enumerate((place, target)):
            for size, index in zip(sizes, where):
                flat[k] = flat[k] * size + index
        pairs.append(tuple(flat))
    return lax.ppermute(value, names, pairs)


def turn_by_core(value, axis):
    size = lax.axis_size(axis)
    pairs = [
        (2 * i + core, 2 * ((i + 1 - 2 * core) % size) + core) for i in range(size) for core in range(2)
    ]
    return lax.ppermute(value, (axis, "core"), pairs)


def from_everyone(shard, axis):
    copies = jnp.broadcast_to(shard, (lax.axis_size(axis), *shard.shape))
    return lax.all_to_all(copies, axis, split_axis=0, concat_axis=0, tiled=True)


def modulation_vectors(condition, context_condition, modulation):
    rows_block = modulation.shape[1]
    silu_pair = jax.nn.silu(jnp.stack([condition, context_condition])).astype(BF16)
    own_rows = lax.dynamic_slice_in_dim(silu_pair, lax.axis_index(SP) * rows_block, rows_block, 1)
    partial_mod = jnp.einsum("cd,rde->cre", own_rows, modulation, preferred_element_type=F32)
    partial_mod = partial_mod.reshape(-1, partial_mod.shape[-1])[:5]
    summed = jnp.sum(from_everyone(partial_mod, SP), axis=0)
    gathered = from_everyone(summed, TP)
    return jnp.moveaxis(gathered, 0, 1).reshape(5, -1)


def rope_tables(rows_own, width):
    z_size = lax.axis_size("z")
    lane = jnp.arange(width)
    eighth = width // 8
    inverse = ROPE_BASE ** (-(lane % eighth).astype(F32) / eighth)
    row = lax.axis_index(SP) * z_size + (lax.axis_index("z") + jnp.arange(z_size)) % z_size
    col = lax.axis_index("core") * rows_own + jnp.arange(rows_own)
    angles = jnp.concatenate([row, col]).astype(F32)[:, None] * inverse
    by_row = (lane % (width // 2)) < width // 4

    def spread(table):
        full = jnp.where(by_row, table[:z_size, None, :], table[None, z_size:, :])
        return full.reshape(z_size * rows_own, width)

    return spread(jnp.cos(angles)), spread(jnp.sin(angles))


def swap_matrix(width):
    source = jnp.arange(width)[:, None]
    target = jnp.arange(width)[None, :]
    eighth = width // 8
    low = target % (2 * eighth) < eighth
    minus = (source == target + eighth) & low
    plus = (source == target - eighth) & ~low
    return plus.astype(BF16) - minus.astype(BF16)


def project(pieces, context, core, vectors, weights, cosine, sine, swap):
    model = vectors.shape[1]
    width = weights[0].shape[1]
    piece_rows = pieces[0].shape[0]
    rows = piece_rows * len(pieces)
    share = context.shape[0] // 2
    total = rows + share
    count = len(pieces)
    step = 16

    def kernel(*refs):
        core_ref, vec, cos_ref, sin_ref, swap_ref = refs[:5]
        token_refs = refs[5 : 5 + count]
        context_ref = refs[5 + count]
        weight_refs = refs[6 + count : 12 + count]
        q_own, kv_own, q_far, kv_far = refs[12 + count : 16 + count]
        tokens, buffer, normed, raw, token_sems, sems = refs[16 + count :]
        copies = [
            pltpu.make_async_copy(
                ref, tokens.at[pl.ds(i * piece_rows, piece_rows)], token_sems.at[i]
            )
            for i, ref in enumerate(token_refs)
        ]
        copies.append(
            pltpu.make_async_copy(
                context_ref.at[pl.ds(core_ref[0] * share, share)],
                tokens.at[pl.ds(rows, share)],
                token_sems.at[count],
            )
        )
        for copy in copies:
            copy.start()
        weight_copies = [
            pltpu.make_async_copy(
                ref, buffer.at[j // 3, :, pl.ds(j % 3 * width, width)], sems.at[j]
            )
            for j, ref in enumerate(weight_refs)
        ]
        for copy in weight_copies:
            copy.start()
        for copy in copies:
            copy.wait()

        def normalize(start, base):
            values = tokens[pl.ds(start, step), :].astype(F32)
            center = jnp.mean(values, axis=-1, keepdims=True)
            shifted = values - center
            spread = jnp.mean(shifted * shifted, axis=-1, keepdims=True)
            out = shifted * lax.rsqrt(spread + EPSILON)
            out = out * (1.0 + vec[base + 1 : base + 2, :]) + vec[base : base + 1, :]
            normed[pl.ds(start, step), :] = out.astype(BF16)

        def one_step(i, carry):
            normalize(pl.multiple_of(i * step, step), 0)
            return carry

        lax.fori_loop(0, rows // step, one_step, 0)
        for low in range(rows, total, step):
            normalize(low, 3)

        def turn(value):
            turned = jnp.dot(value, swap_ref[...], preferred_element_type=F32)
            return (value.astype(F32) * cos_ref[...] + turned * sin_ref[...]).astype(BF16)

        for head, q_ref, kv_ref in ((1, q_far, kv_far), (0, q_own, kv_own)):
            for j in range(3):
                weight_copies[3 * head + j].wait()
            raw[...] = jnp.dot(normed[...], buffer[head], preferred_element_type=F32).astype(BF16)
            q_ref[...] = turn(raw[:rows, :width])
            kv_ref[0, :rows, :] = turn(raw[:rows, width : 2 * width])
            kv_ref[0, rows:, :] = raw[rows:, width : 2 * width]
            kv_ref[1, :, :] = raw[:, 2 * width :]

    vmem = pl.BlockSpec(memory_space=pltpu.VMEM)
    anywhere = pl.BlockSpec(memory_space=ANY)
    shapes = [(rows, width), (2, total, width)] * 2
    return pl.pallas_call(
        kernel,
        out_shape=[jax.ShapeDtypeStruct(shape, BF16) for shape in shapes],
        in_specs=[pl.BlockSpec(memory_space=pltpu.SMEM)] + [vmem] * 4 + [anywhere] * (count + 7),
        out_specs=[vmem] * 4,
        scratch_shapes=[
            pltpu.VMEM((total, model), BF16),
            pltpu.VMEM((2, model, 3 * width), BF16),
            pltpu.VMEM((total, model), BF16),
            pltpu.VMEM((total, 3 * width), BF16),
            pltpu.SemaphoreType.DMA((count + 1,)),
            pltpu.SemaphoreType.DMA((6,)),
        ],
        cost_estimate=pl.CostEstimate(
            flops=2 * 6 * total * model * width, bytes_accessed=12 * model * width, transcendentals=0
        ),
        name="project",
    )(core, vectors, cosine, sine, swap, *pieces, context, *weights)


def attend(queries, arrays, lift, state=None, final=None, payload=False):
    query_a, query_b = queries
    rows, width = query_a.shape
    half = width // 2
    number = len(arrays)
    total = arrays[0].shape[-2]
    scale = half ** (-0.5) * LOG2E
    first, last = state is None, final is not None
    others = final[2] if last else ()
    group = 2

    def kernel(*refs):
        lift_ref, qa_ref, qb_ref = refs[:3]
        key_refs = refs[3 : 3 + number]
        rest = refs[3 + number :]
        if not first:
            m_in, l_in, o_in = rest[:3]
            rest = rest[3:]
        if last:
            lambda_ref, gain_ref = rest[:2]
            other_refs = rest[2 : 2 + len(others)]
            out_ref, scores, accs = rest[2 + len(others) :]
        elif payload:
            out_ref, scores, accs = rest
        else:
            m_out, l_out, o_out, scores, accs = rest
        lift_two = lift_ref[0] * LOG2E
        which = pl.program_id(0)

        @pl.when(which == 0)
        def _():
            accs[2] = qa_ref[...].astype(F32)

        @pl.when(which == 1)
        def _():
            accs[2] = qb_ref[...].astype(F32)

        query = accs[2].astype(BF16)
        tops, lifteds = [], []
        for m in range(2):
            left, right = m * half, (m + 1) * half
            q = query[:, left:right]
            peak = None
            for u, ref in enumerate(key_refs):
                keys = ref[0, :rows, left:right]
                block = lax.dot_general(q, keys, (((1,), (1,)), ((), ())), preferred_element_type=F32)
                scores[m, :, u * rows : (u + 1) * rows] = block
                for lane in range(0, rows, 128):
                    piece = block[:, lane : lane + 128]
                    peak = piece if peak is None else jnp.maximum(peak, piece)
            keys = jnp.concatenate([ref[0, rows:total, left:right] for ref in key_refs], axis=0)
            lifted = lax.dot_general(q, keys, (((1,), (1,)), ((), ())), preferred_element_type=F32)
            lifted = lifted * scale + lift_two
            top = jnp.max(peak, axis=1, keepdims=True) * scale
            tops.append(jnp.maximum(top, jnp.max(lifted, axis=1, keepdims=True)))
            lifteds.append(lifted)
        outs, logs = [], []
        for m in range(2):
            new, lifted = tops[m], lifteds[m]
            if first:
                total_sum = None
                before = None
            else:
                old = m_in[m, 0, :, :1]
                new = jnp.maximum(old, new)
                fading = jnp.exp2(old - new)
                total_sum = l_in[m, 0] * fading
                before = o_in[m, 0] * fading
            values = jnp.concatenate([ref[1, rows:total, :] for ref in key_refs], axis=0)
            weights = jnp.exp2(lifted - new)
            extra = jnp.sum(weights, axis=1, keepdims=True)
            product = jnp.dot(weights.astype(BF16), values, preferred_element_type=F32)
            accs[m] = product if before is None else before + product
            for u in range(0, number, group):
                weights = jnp.exp2(scores[m, :, u * rows : (u + group) * rows] * scale - new)
                for lane in range(0, group * rows, 128):
                    piece = weights[:, lane : lane + 128]
                    total_sum = piece if total_sum is None else total_sum + piece
                values = jnp.concatenate([ref[1, :rows, :] for ref in key_refs[u : u + group]], axis=0)
                accs[m] += jnp.dot(weights.astype(BF16), values, preferred_element_type=F32)
            if not last and not payload:
                lanes = lax.broadcasted_iota(jnp.int32, total_sum.shape, 1)
                l_out[m, 0] = total_sum + jnp.where(lanes == 0, extra, 0.0)
                m_out[m, 0] = jnp.broadcast_to(new, total_sum.shape)
                o_out[m, 0] = accs[m]
                continue
            row_sums = jnp.sum(total_sum, axis=1, keepdims=True) + extra
            outs.append(accs[m] / row_sums)
            logs.append(new + jnp.log(row_sums) * LOG2E)
        if payload:
            lanes = lax.broadcasted_iota(jnp.int32, (rows, 128), 1)
            plane = jnp.zeros((rows, 128), F32)
            for m in range(2):
                out_ref[2 * m, 0] = outs[m][:, :128].astype(BF16)
                out_ref[2 * m + 1, 0] = outs[m][:, 128:].astype(BF16)
                left_over = logs[m]
                for k in range(3):
                    piece = left_over.astype(BF16).astype(F32)
                    plane = jnp.where(lanes == 3 * m + k, piece, plane)
                    left_over = left_over - piece
            out_ref[4, 0] = plane.astype(BF16)
        if last:
            merged = []
            for m in range(2):
                parts, sizes = [outs[m]], [logs[m]]
                for ref in other_refs:
                    parts.append(
                        jnp.concatenate([ref[2 * m, 0], ref[2 * m + 1, 0]], axis=1).astype(F32)
                    )
                    plane = ref[4, 0].astype(F32)
                    low = 3 * m
                    sizes.append(
                        plane[:, low : low + 1] + plane[:, low + 1 : low + 2] + plane[:, low + 2 : low + 3]
                    )
                top = functools.reduce(jnp.maximum, sizes)
                shares = [jnp.exp2(size - top) for size in sizes]
                whole_sum = functools.reduce(jnp.add, shares)
                out = functools.reduce(jnp.add, [s * part for s, part in zip(shares, parts)])
                merged.append(out / whole_sum)
            difference = merged[0] - lambda_ref[0] * merged[1]
            power = jnp.mean(difference * difference, axis=1, keepdims=True)
            out_ref[0] = (difference * lax.rsqrt(power + EPSILON) * gain_ref[...]).astype(BF16)

    smem = pl.BlockSpec(memory_space=pltpu.SMEM)

    def whole(array):
        return pl.BlockSpec(array.shape, lambda i, dims=array.ndim: (0,) * dims)

    narrow = pl.BlockSpec((2, 1, rows, 128), lambda i: (0, i, 0, 0))
    wide = pl.BlockSpec((2, 1, rows, width), lambda i: (0, i, 0, 0))
    planes = pl.BlockSpec((5, 1, rows, 128), lambda i: (0, i, 0, 0))
    inputs = [lift, query_a, query_b, *arrays]
    in_specs = [smem, whole(query_a), whole(query_b), *(whole(array) for array in arrays)]
    if not first:
        inputs += list(state)
        in_specs += [narrow, narrow, wide]
    if last:
        lambdas, gain, _ = final
        inputs += [lambdas, gain, *others]
        in_specs += [smem, whole(gain), *([planes] * len(others))]
        out_shape = jax.ShapeDtypeStruct((2, rows, width), BF16)
        out_specs = pl.BlockSpec((1, rows, width), lambda i: (i, 0, 0))
    elif payload:
        out_shape = jax.ShapeDtypeStruct((5, 2, rows, 128), BF16)
        out_specs = planes
    else:
        out_shape = [
            jax.ShapeDtypeStruct((2, 2, rows, 128), F32),
            jax.ShapeDtypeStruct((2, 2, rows, 128), F32),
            jax.ShapeDtypeStruct((2, 2, rows, width), F32),
        ]
        out_specs = [narrow, narrow, wide]
    return pl.pallas_call(
        kernel,
        grid=(2,),
        out_shape=out_shape,
        in_specs=in_specs,
        out_specs=out_specs,
        scratch_shapes=[
            pltpu.VMEM((2, rows, number * rows), F32),
            pltpu.VMEM((3, rows, width), F32),
        ],
        cost_estimate=pl.CostEstimate(
            flops=2 * 12 * rows * number * total * half,
            bytes_accessed=4 * number * total * width,
            transcendentals=4 * rows * number * total,
        ),
        name="attend",
    )(*inputs)


def output_product(own, far, weight_own, weight_far):
    rows, width = own.shape
    model = weight_own.shape[1]
    block = 512

    def kernel(own_ref, far_ref, a_ref, b_ref, out_ref):
        def one(i, carry):
            place = pl.ds(pl.multiple_of(i * block, block), block)
            product = jnp.dot(own_ref[...], a_ref[:, place], preferred_element_type=F32)
            product += jnp.dot(far_ref[...], b_ref[:, place], preferred_element_type=F32)
            out_ref[:, place] = product.astype(BF16)
            return carry

        lax.fori_loop(0, model // block, one, 0)

    vmem = pl.BlockSpec(memory_space=pltpu.VMEM)
    return pl.pallas_call(
        kernel,
        out_shape=jax.ShapeDtypeStruct((rows, model), BF16),
        in_specs=[vmem] * 4,
        out_specs=vmem,
        cost_estimate=pl.CostEstimate(
            flops=4 * rows * width * model, bytes_accessed=4 * width * model, transcendentals=0
        ),
        name="output_product",
    )(own, far, weight_own, weight_far)


def plus(first, second):
    return (first.astype(F32) + second.astype(F32)).astype(BF16)


def shards(
    latent,
    context,
    condition,
    context_condition,
    modulation,
    query_weight,
    key_weight,
    value_weight,
    lambdas,
    context_lift,
    head_gain,
    output_weight,
):
    core = lax.axis_index("core")
    up1, down1 = hop(latent, "z", 1), hop(latent, "z", -1)
    up2, down2 = hop(up1, "z", 1), hop(down1, "z", -1)
    up3, down3 = hop(up2, "z", 1), hop(down2, "z", -1)
    opposite = turn_by_core(jnp.where(core == 0, up3, down3), "z")
    pieces = [latent, down1, down2, down3, opposite, up3, up2, up1]

    own_weights = [query_weight, key_weight, value_weight]
    far_weights = [hop(weight, "core", 1) for weight in own_weights]
    far_output = hop(output_weight, "core", 1)

    vectors = modulation_vectors(condition, context_condition, modulation)
    cosine, sine = rope_tables(latent.shape[0], query_weight.shape[1])
    swap = swap_matrix(query_weight.shape[1])

    q_a, kv_a, q_send, kv_send = project(
        pieces, context, core[None], vectors, own_weights + far_weights, cosine, sine, swap
    )
    kv_b = hop(kv_send, "core", 1)
    q_b = hop(q_send, "core", 1)

    def across(value, step):
        return hop_by_core(value, ("x", "y"), step)

    def along(value, step):
        return hop_by_core(value, ("y", "x"), step)

    a_p, a_m = along(kv_a, 1), along(kv_a, -1)
    qa_p, qa_m = across(q_a, 1), across(q_a, -1)
    b_p, b_m = along(kv_b, 1), along(kv_b, -1)
    qb_p, qb_m = across(q_b, 1), across(q_b, -1)
    a_2, b_2 = along(a_p, 1), along(b_m, -1)
    qa_2, qb_2 = across(qa_p, 1), across(qb_m, -1)

    near = [kv_a, kv_b, a_p, b_p, a_m, b_m]
    state = attend((q_a, q_b), near, context_lift)
    far = attend((qa_2, qb_2), near + [a_2, b_2], context_lift, payload=True)
    from_2 = across(far, 2)
    after = attend((qa_p, qb_p), near + [a_2, b_2], context_lift, payload=True)
    from_m = across(after, -1)
    ahead = attend((qa_m, qb_m), near + [a_2, b_2], context_lift, payload=True)
    from_p = across(ahead, 1)
    attended = attend(
        (q_a, q_b),
        [a_2, b_2],
        context_lift,
        state,
        (lambdas, head_gain[None], (from_2, from_m, from_p)),
    )

    far_heads = hop(attended[1], "core", 1)
    product = output_product(attended[0], far_heads, output_weight, far_output)
    share = product.reshape(-1, *latent.shape)
    arrived = turn_by_core(share[4], "z").astype(F32)
    up = share[3].astype(F32) + jnp.where(core == 0, arrived, 0.0)
    down = share[5].astype(F32) + jnp.where(core == 0, 0.0, arrived)
    up, down = hop(up.astype(BF16), "z", 1), hop(down.astype(BF16), "z", -1)
    up, down = hop(plus(share[2], up), "z", 1), hop(plus(share[6], down), "z", -1)
    up, down = hop(plus(share[1], up), "z", 1), hop(plus(share[7], down), "z", -1)
    mixture = share[0].astype(F32) + up.astype(F32) + down.astype(F32)
    return (latent.astype(F32) + vectors[2] * mixture).astype(BF16)


def solution(mesh):
    split = Mesh(mesh.devices.reshape(4, 4, mesh.shape["tp"] // 2, 2), ALL)
    return jax.shard_map(
        shards,
        mesh=split,
        in_specs=(
            P(ALL, None),
            P(SP, None),
            P(),
            P(),
            P(None, SP, TP),
            P(None, TP),
            P(None, TP),
            P(None, TP),
            P(TP),
            P(TP),
            P(),
            P(TP, None),
        ),
        out_specs=P(ALL, None),
        check_vma=False,
    )
```

```python
import functools
import itertools
import math

import jax
import jax.numpy as jnp
from jax import lax
from jax.experimental import pallas as pl
from jax.experimental.pallas import tpu as pltpu
from jax.sharding import Mesh
from jax.sharding import PartitionSpec as P

ROPE_BASE = 10000.0
EPSILON = 1e-05
LOG2E = math.log2(math.e)
SP = ("y", "x")
TP = ("z", "core")
ALL = SP + TP
F32 = jnp.float32
BF16 = jnp.bfloat16
JOINED = False
UNROLL = 4
OUT_BLOCK = 1024
OUT_UNROLL = 2


def hop(value, axis, step):
    size = lax.axis_size(axis)
    return lax.ppermute(value, axis, [(i, (i + step) % size) for i in range(size)])


def hop_by_core(value, axes, step):
    names = tuple(name for name in ALL if name in (*axes, "core"))
    sizes = [lax.axis_size(name) for name in names]
    pairs = []
    for place in itertools.product(*(range(size) for size in sizes)):
        target = list(place)
        at = names.index(axes[place[names.index("core")]])
        target[at] = (target[at] + step) % sizes[at]
        flat = [0, 0]
        for k, where in enumerate((place, target)):
            for size, index in zip(sizes, where):
                flat[k] = flat[k] * size + index
        pairs.append(tuple(flat))
    return lax.ppermute(value, names, pairs)


def turn_by_core(value, axis):
    size = lax.axis_size(axis)
    pairs = [
        (2 * i + core, 2 * ((i + 1 - 2 * core) % size) + core) for i in range(size) for core in range(2)
    ]
    return lax.ppermute(value, (axis, "core"), pairs)


def from_everyone(shard, axis):
    copies = jnp.broadcast_to(shard, (lax.axis_size(axis), *shard.shape))
    return lax.all_to_all(copies, axis, split_axis=0, concat_axis=0, tiled=True)


def modulation_columns(condition, context_condition, modulation):
    rows_block = modulation.shape[1]
    silu_pair = jax.nn.silu(jnp.stack([condition, context_condition])).astype(BF16)
    own_rows = lax.dynamic_slice_in_dim(silu_pair, lax.axis_index(SP) * rows_block, rows_block, 1)
    partial_mod = jnp.einsum("cd,rde->cre", own_rows, modulation, preferred_element_type=F32)
    partial_mod = partial_mod.reshape(-1, partial_mod.shape[-1])[:5]
    return jnp.sum(from_everyone(partial_mod, SP), axis=0)


def rope_tables(rows_own, width, offsets):
    z_size = lax.axis_size("z")
    lane = jnp.arange(width)
    eighth = width // 8
    inverse = ROPE_BASE ** (-(lane % eighth).astype(F32) / eighth)
    row = lax.axis_index(SP) * z_size + (lax.axis_index("z") + offsets) % z_size
    col = lax.axis_index("core") * rows_own + jnp.arange(rows_own)
    angles = jnp.concatenate([row, col]).astype(F32)[:, None] * inverse
    by_row = (lane % (width // 2)) < width // 4

    def spread(table):
        full = jnp.where(by_row, table[:z_size, None, :], table[None, z_size:, :])
        return full.reshape(z_size * rows_own, width)

    return spread(jnp.cos(angles)), spread(jnp.sin(angles))


def swap_matrix(width):
    source = jnp.arange(width)[:, None]
    target = jnp.arange(width)[None, :]
    eighth = width // 8
    low = target % (2 * eighth) < eighth
    minus = (source == target + eighth) & low
    plus = (source == target - eighth) & ~low
    return plus.astype(BF16) - minus.astype(BF16)


def project(pieces, context, place, vectors, weights, cosine, sine, swap):
    model = vectors.shape[1]
    width = weights[0].shape[1]
    piece_rows = pieces[0].shape[0]
    rows = piece_rows * len(pieces)
    share = context.shape[0] // 2
    total = rows + share
    count = len(pieces)
    step = 16

    def kernel(*refs):
        place_ref, vec, cos_ref, sin_ref, swap_ref = refs[:5]
        token_refs = refs[5 : 5 + count]
        context_ref = refs[5 + count]
        weight_refs = refs[6 + count : 12 + count]
        q_own, kv_own, q_far, kv_far = refs[12 + count : 16 + count]
        tokens, buffer, normed, raw, sems = refs[16 + count :]
        weight_copies = [
            pltpu.make_async_copy(
                ref, buffer.at[j // 3, :, pl.ds(j % 3 * width, width)], sems.at[j]
            )
            if JOINED
            else pltpu.make_async_copy(ref, buffer.at[j], sems.at[j])
            for j, ref in enumerate(weight_refs)
        ]
        for copy in weight_copies[3:] + weight_copies[:3]:
            copy.start()
        for i, ref in enumerate(token_refs):
            slot = pl.multiple_of(place_ref[i + 1] * piece_rows, piece_rows)
            tokens[pl.ds(slot, piece_rows), :] = ref[...]
        low = pl.multiple_of(place_ref[0] * share, share)
        tokens[rows:, :] = context_ref[pl.ds(low, share), :]

        def normalize(start, base):
            values = tokens[pl.ds(start, step), :].astype(F32)
            center = jnp.mean(values, axis=-1, keepdims=True)
            shifted = values - center
            spread = jnp.mean(shifted * shifted, axis=-1, keepdims=True)
            out = shifted * lax.rsqrt(spread + EPSILON)
            out = out * (1.0 + vec[base + 1 : base + 2, :]) + vec[base : base + 1, :]
            normed[pl.ds(start, step), :] = out.astype(BF16)

        def one_step(i, carry):
            normalize(pl.multiple_of(i * step, step), 0)
            return carry

        lax.fori_loop(0, rows // step, one_step, 0, unroll=UNROLL)
        for low in range(rows, total, step):
            normalize(low, 3)

        def turn(value):
            turned = jnp.dot(value, swap_ref[...], preferred_element_type=F32)
            return (value.astype(F32) * cos_ref[...] + turned * sin_ref[...]).astype(BF16)

        for head, q_ref, kv_ref in ((1, q_far, kv_far), (0, q_own, kv_own)):
            for j in range(3):
                weight_copies[3 * head + j].wait()
                if not JOINED:
                    raw[:, j * width : (j + 1) * width] = jnp.dot(
                        normed[...], buffer[3 * head + j], preferred_element_type=F32
                    ).astype(BF16)
            if JOINED:
                raw[...] = jnp.dot(normed[...], buffer[head], preferred_element_type=F32).astype(BF16)
            q_ref[...] = turn(raw[:rows, :width])
            kv_ref[0, :rows, :] = turn(raw[:rows, width : 2 * width])
            kv_ref[0, rows:, :] = raw[rows:, width : 2 * width]
            kv_ref[1, :, :] = raw[:, 2 * width :]

    vmem = pl.BlockSpec(memory_space=pltpu.VMEM)
    shapes = [(rows, width), (2, total, width)] * 2
    return pl.pallas_call(
        kernel,
        out_shape=[jax.ShapeDtypeStruct(shape, BF16) for shape in shapes],
        in_specs=[pl.BlockSpec(memory_space=pltpu.SMEM)] + [vmem] * (count + 5)
        + [pl.BlockSpec(memory_space=pltpu.HBM)] * 6,
        out_specs=[vmem] * 4,
        scratch_shapes=[
            pltpu.VMEM((total, model), BF16),
            pltpu.VMEM((2, model, 3 * width) if JOINED else (6, model, width), BF16),
            pltpu.VMEM((total, model), BF16),
            pltpu.VMEM((total, 3 * width), BF16),
            pltpu.SemaphoreType.DMA((6,)),
        ],
        cost_estimate=pl.CostEstimate(
            flops=2 * 6 * total * model * width, bytes_accessed=12 * model * width, transcendentals=0
        ),
        name="project",
    )(place, vectors, cosine, sine, swap, *pieces, context, *weights)


def join(pairs):
    def kernel(*refs):
        number = 2 * len(pairs)
        for i, ref in enumerate(refs[:number]):
            refs[number + i // 2][i % 2] = ref[...]

    vmem = pl.BlockSpec(memory_space=pltpu.VMEM)
    return pl.pallas_call(
        kernel,
        out_shape=[jax.ShapeDtypeStruct((2, *first.shape), first.dtype) for first, _ in pairs],
        in_specs=[vmem] * (2 * len(pairs)),
        out_specs=[vmem] * len(pairs),
        name="join",
    )(*(array for pair in pairs for array in pair))


def attend(queries, arrays, lift, state=None, final=None, payload=False):
    _, rows, width = queries.shape
    half = width // 2
    number = 2 * len(arrays)
    total = arrays[0].shape[-2]
    scale = half ** (-0.5) * LOG2E
    first, last = state is None, final is not None
    others = final[2] if last else ()
    group = 2

    def kernel(*refs):
        lift_ref, q_ref = refs[:2]
        key_refs = [ref.at[i] for ref in refs[2 : 2 + len(arrays)] for i in range(2)]
        rest = refs[2 + len(arrays) :]
        if not first:
            m_in, l_in, o_in = rest[:3]
            rest = rest[3:]
        if last:
            lambda_ref, gain_ref = rest[:2]
            other_refs = rest[2 : 2 + len(others)]
            out_mine, out_core, out_chip, out_both, scores, accs = rest[2 + len(others) :]
        elif payload:
            out_ref, scores, accs = rest
        else:
            m_out, l_out, o_out, scores, accs = rest
        lift_two = lift_ref[0] * LOG2E
        query = q_ref[0]
        tops, lifteds = [], []
        for m in range(2):
            left, right = m * half, (m + 1) * half
            q = query[:, left:right]
            peak = None
            for u, ref in enumerate(key_refs):
                keys = ref[0, :rows, left:right]
                block = lax.dot_general(q, keys, (((1,), (1,)), ((), ())), preferred_element_type=F32)
                scores[m, :, u * rows : (u + 1) * rows] = block
                for lane in range(0, rows, 128):
                    piece = block[:, lane : lane + 128]
                    peak = piece if peak is None else jnp.maximum(peak, piece)
            keys = jnp.concatenate([ref[0, rows:total, left:right] for ref in key_refs], axis=0)
            lifted = lax.dot_general(q, keys, (((1,), (1,)), ((), ())), preferred_element_type=F32)
            lifted = lifted * scale + lift_two
            top = jnp.max(peak, axis=1, keepdims=True) * scale
            tops.append(jnp.maximum(top, jnp.max(lifted, axis=1, keepdims=True)))
            lifteds.append(lifted)
        outs, logs = [], []
        for m in range(2):
            new, lifted = tops[m], lifteds[m]
            if first:
                total_sum = None
                before = None
            else:
                old = m_in[m, 0, :, :1]
                new = jnp.maximum(old, new)
                fading = jnp.exp2(old - new)
                total_sum = l_in[m, 0] * fading
                before = o_in[m, 0] * fading
            values = jnp.concatenate([ref[1, rows:total, :] for ref in key_refs], axis=0)
            weights = jnp.exp2(lifted - new)
            extra = jnp.sum(weights, axis=1, keepdims=True)
            product = jnp.dot(weights.astype(BF16), values, preferred_element_type=F32)
            accs[m] = product if before is None else before + product
            for u in range(0, number, group):
                weights = jnp.exp2(scores[m, :, u * rows : (u + group) * rows] * scale - new)
                for lane in range(0, group * rows, 128):
                    piece = weights[:, lane : lane + 128]
                    total_sum = piece if total_sum is None else total_sum + piece
                values = jnp.concatenate([ref[1, :rows, :] for ref in key_refs[u : u + group]], axis=0)
                accs[m] += jnp.dot(weights.astype(BF16), values, preferred_element_type=F32)
            if not last and not payload:
                lanes = lax.broadcasted_iota(jnp.int32, total_sum.shape, 1)
                l_out[m, 0] = total_sum + jnp.where(lanes == 0, extra, 0.0)
                m_out[m, 0] = jnp.broadcast_to(new, total_sum.shape)
                o_out[m, 0] = accs[m]
                continue
            row_sums = jnp.sum(total_sum, axis=1, keepdims=True) + extra
            outs.append(accs[m] / row_sums)
            logs.append(new + jnp.log(row_sums) * LOG2E)
        if payload:
            lanes = lax.broadcasted_iota(jnp.int32, (rows, 128), 1)
            plane = jnp.zeros((rows, 128), F32)
            for m in range(2):
                out_ref[2 * m, 0] = outs[m][:, :128].astype(BF16)
                out_ref[2 * m + 1, 0] = outs[m][:, 128:].astype(BF16)
                left_over = logs[m]
                for k in range(3):
                    piece = left_over.astype(BF16).astype(F32)
                    plane = jnp.where(lanes == 3 * m + k, piece, plane)
                    left_over = left_over - piece
            out_ref[4, 0] = plane.astype(BF16)
        if last:
            source = lax.broadcasted_iota(jnp.int32, (128, width), 0)
            target = lax.broadcasted_iota(jnp.int32, (128, width), 1)
            spread = (source // 3 == target // 128).astype(BF16)
            sizes = [
                jnp.dot(ref[4, 0], spread, preferred_element_type=F32) for ref in other_refs
            ]
            merged = []
            for m in range(2):
                sizes_m = [jnp.broadcast_to(logs[m], (rows, 128))]
                sizes_m += [size[:, m * 128 : (m + 1) * 128] for size in sizes]
                top = functools.reduce(jnp.maximum, sizes_m)
                shares = [jnp.exp2(size - top) for size in sizes_m]
                inverse = 1.0 / functools.reduce(jnp.add, shares)
                pieces = []
                for k in range(2):
                    out = shares[0] * outs[m][:, k * 128 : (k + 1) * 128]
                    for share, ref in zip(shares[1:], other_refs):
                        out = out + share * ref[2 * m + k, 0].astype(F32)
                    pieces.append(out * inverse)
                merged.append(jnp.concatenate(pieces, axis=1))
            difference = merged[0] - lambda_ref[0] * merged[1]
            power = jnp.mean(difference * difference, axis=1, keepdims=True)
            head = (difference * lax.rsqrt(power + EPSILON) * gain_ref[...]).astype(BF16)

            @pl.when(pl.program_id(0) == 0)
            def _():
                out_mine[...] = head[: rows // 2]
                out_chip[...] = head[rows // 2 :]

            @pl.when(pl.program_id(0) == 1)
            def _():
                out_core[...] = head[: rows // 2]
                out_both[...] = head[rows // 2 :]

    smem = pl.BlockSpec(memory_space=pltpu.SMEM)

    def whole(array):
        return pl.BlockSpec(array.shape, lambda i, dims=array.ndim: (0,) * dims)

    narrow = pl.BlockSpec((2, 1, rows, 128), lambda i: (0, i, 0, 0))
    wide = pl.BlockSpec((2, 1, rows, width), lambda i: (0, i, 0, 0))
    planes = pl.BlockSpec((5, 1, rows, 128), lambda i: (0, i, 0, 0))
    inputs = [lift, queries, *arrays]
    by_query = pl.BlockSpec((1, rows, width), lambda i: (i, 0, 0))
    in_specs = [smem, by_query, *(whole(array) for array in arrays)]
    if not first:
        inputs += list(state)
        in_specs += [narrow, narrow, wide]
    if last:
        lambdas, gain, _ = final
        inputs += [lambdas, gain, *others]
        in_specs += [smem, whole(gain), *([planes] * len(others))]
        out_shape = [jax.ShapeDtypeStruct((rows // 2, width), BF16)] * 4
        out_specs = [pl.BlockSpec((rows // 2, width), lambda i: (0, 0))] * 4
    elif payload:
        out_shape = jax.ShapeDtypeStruct((5, 2, rows, 128), BF16)
        out_specs = planes
    else:
        out_shape = [
            jax.ShapeDtypeStruct((2, 2, rows, 128), F32),
            jax.ShapeDtypeStruct((2, 2, rows, 128), F32),
            jax.ShapeDtypeStruct((2, 2, rows, width), F32),
        ]
        out_specs = [narrow, narrow, wide]
    return pl.pallas_call(
        kernel,
        grid=(2,),
        out_shape=out_shape,
        in_specs=in_specs,
        out_specs=out_specs,
        scratch_shapes=[
            pltpu.VMEM((2, rows, number * rows), F32),
            pltpu.VMEM((2, rows, width), F32),
        ],
        cost_estimate=pl.CostEstimate(
            flops=2 * 12 * rows * number * total * half,
            bytes_accessed=4 * number * total * width,
            transcendentals=4 * rows * number * total,
        ),
        name="attend",
    )(*inputs)


def output_product(heads, weights):
    rows, width = heads[0].shape
    model = weights[0].shape[1]
    parts = 4
    part = rows // parts
    number = len(heads)

    def kernel(*refs):
        outs = refs[2 * number :]

        def one(i, carry):
            place = pl.ds(pl.multiple_of(i * OUT_BLOCK, OUT_BLOCK), OUT_BLOCK)
            product = None
            for j in range(number):
                term = jnp.dot(refs[j][...], refs[number + j][:, place], preferred_element_type=F32)
                product = term if product is None else product + term
            for k in range(parts):
                outs[k][:, place] = product[k * part : (k + 1) * part].astype(BF16)
            return carry

        lax.fori_loop(0, model // OUT_BLOCK, one, 0, unroll=OUT_UNROLL)

    vmem = pl.BlockSpec(memory_space=pltpu.VMEM)
    return pl.pallas_call(
        kernel,
        out_shape=[jax.ShapeDtypeStruct((part, model), BF16)] * parts,
        in_specs=[vmem] * (2 * number),
        out_specs=[vmem] * parts,
        cost_estimate=pl.CostEstimate(
            flops=2 * number * rows * width * model,
            bytes_accessed=2 * number * width * model,
            transcendentals=0,
        ),
        name="output_product",
    )(*heads, *weights)


def hop_by_parity(value, axis, step_even, step_odd):
    size = lax.axis_size(axis)
    return lax.ppermute(
        value, axis, [(i, (i + (step_odd if i % 2 else step_even)) % size) for i in range(size)]
    )


def plus(first, second):
    return (first.astype(F32) + second.astype(F32)).astype(BF16)


def steps(
    latent,
    context,
    condition,
    context_condition,
    modulation,
    query_weight,
    key_weight,
    value_weight,
    lambdas,
    context_lift,
    head_gain,
    output_weight,
):
    core = lax.axis_index("core")
    odd = lax.axis_index("z") % 2
    up1, down1 = hop(latent, "z", 1), hop(latent, "z", -1)
    down2 = hop(down1, "z", -1)
    up2 = hop(up1, "z", 1)
    columns = modulation_columns(condition, context_condition, modulation)
    gathered = from_everyone(columns, TP)
    up3, down3 = hop(up2, "z", 1), hop(down2, "z", -1)
    gathered, up3, down3 = lax.optimization_barrier((gathered, up3, down3))
    vectors = jnp.moveaxis(gathered, 0, 1).reshape(5, -1)
    opposite = turn_by_core(jnp.where(core == 0, up3, down3), "z")
    pieces = [latent, up1, up2, up3, down1, down2, down3, opposite]
    sign = 2 * odd - 1
    blocks = jnp.arange(8)
    offsets = jnp.where(blocks < 4, sign * blocks, sign * (3 - blocks))
    place = jnp.concatenate(
        [core[None], jnp.array([0, 1, 2, 3, 4, 5, 6, 7]) + jnp.array([0, 3, 3, 3, -3, -3, -3, 0]) * odd]
    ).astype(jnp.int32)

    own_weights = [query_weight, key_weight, value_weight]
    far_weights = [hop(weight, "core", 1) for weight in own_weights]
    core_output = hop(output_weight, "core", 1)
    cosine, sine = rope_tables(latent.shape[0], query_weight.shape[1], offsets)
    swap = swap_matrix(query_weight.shape[1])

    q_a, kv_a, q_send, kv_send = project(
        pieces, context, place, vectors, own_weights + far_weights, cosine, sine, swap
    )
    kv_b = hop(kv_send, "core", 1)
    q_b = hop(q_send, "core", 1)
    later, q_a = lax.optimization_barrier((output_weight, q_a))
    chip_output = hop_by_parity(later, "z", 1, -1)

    def across(value, step):
        return hop_by_core(value, ("x", "y"), step)

    def along(value, step):
        return hop_by_core(value, ("y", "x"), step)

    kv, queries = join([(kv_a, kv_b), (q_a, q_b)])
    kv_p, kv_m = along(kv, 1), along(kv, -1)
    q_p, q_m = across(queries, 1), across(queries, -1)
    kv_on, q_on = lax.optimization_barrier((kv_p, q_m))
    kv_2 = along(kv_on, 1)
    q_2 = across(q_on, -1)

    near = [kv, kv_p, kv_m]
    state = attend(queries, near, context_lift)
    from_2 = across(attend(q_2, near + [kv_2], context_lift, payload=True), 2)
    from_m = across(attend(q_p, near + [kv_2], context_lift, payload=True), -1)
    ahead = attend(q_m, near + [kv_2], context_lift, payload=True)
    from_p = across(ahead, 1)
    mine, for_core, for_chip, for_both = attend(
        queries, [kv_2], context_lift, state, (lambdas, head_gain[None], (from_2, from_m, from_p))
    )

    later, mine = lax.optimization_barrier((chip_output, mine))
    both_output = hop(later, "core", 1)
    of_both = hop(hop_by_parity(for_both, "z", 1, -1), "core", 1)
    of_chip = hop_by_parity(for_chip, "z", 1, -1)
    of_core = hop(for_core, "core", 1)
    share = output_product(
        [mine, of_core, of_chip, of_both], [output_weight, core_output, chip_output, both_output]
    )
    third = hop_by_parity(share[3], "z", -2, 2)
    second = hop_by_parity(share[2], "z", -2, 2)
    first = hop_by_parity(plus(share[1], third), "z", -1, 1)
    mixture = share[0].astype(F32) + second.astype(F32) + first.astype(F32)
    return (latent.astype(F32) + vectors[2] * mixture).astype(BF16)


def solution(mesh):
    split = Mesh(mesh.devices.reshape(4, 4, mesh.shape["tp"] // 2, 2), ALL)
    return jax.shard_map(
        steps,
        mesh=split,
        in_specs=(
            P(ALL, None),
            P(SP, None),
            P(),
            P(),
            P(None, SP, TP),
            P(None, TP),
            P(None, TP),
            P(None, TP),
            P(TP),
            P(TP),
            P(),
            P(TP, None),
        ),
        out_specs=P(ALL, None),
        check_vma=False,
    )
```

```python
import functools
import itertools
import math

import jax
import jax.numpy as jnp
from jax import lax
from jax.experimental import pallas as pl
from jax.experimental.pallas import tpu as pltpu
from jax.sharding import Mesh
from jax.sharding import PartitionSpec as P

ROPE_BASE = 10000.0
EPSILON = 1e-05
LOG2E = math.log2(math.e)
SP = ("y", "x")
TP = ("z", "core")
ALL = SP + TP
F32 = jnp.float32
BF16 = jnp.bfloat16
UNROLL = 2
OUT_BLOCK = 1024
OUT_UNROLL = 1


def hop(value, axis, step):
    size = lax.axis_size(axis)
    return lax.ppermute(value, axis, [(i, (i + step) % size) for i in range(size)])


def hop_by_core(value, axes, step):
    names = tuple(name for name in ALL if name in (*axes, "core"))
    sizes = [lax.axis_size(name) for name in names]
    pairs = []
    for place in itertools.product(*(range(size) for size in sizes)):
        target = list(place)
        at = names.index(axes[place[names.index("core")]])
        target[at] = (target[at] + step) % sizes[at]
        flat = [0, 0]
        for k, where in enumerate((place, target)):
            for size, index in zip(sizes, where):
                flat[k] = flat[k] * size + index
        pairs.append(tuple(flat))
    return lax.ppermute(value, names, pairs)


def turn_by_core(value, axis, step):
    size = lax.axis_size(axis)
    pairs = [
        (2 * i + core, 2 * ((i + (1 - 2 * core) * step) % size) + core) for i in range(size) for core in range(2)
    ]
    return lax.ppermute(value, (axis, "core"), pairs)


def from_everyone(shard, axis):
    copies = jnp.broadcast_to(shard, (lax.axis_size(axis), *shard.shape))
    return lax.all_to_all(copies, axis, split_axis=0, concat_axis=0, tiled=True)


def modulation_columns(condition, context_condition, modulation):
    rows_block = modulation.shape[1]
    silu_pair = jax.nn.silu(jnp.stack([condition, context_condition])).astype(BF16)
    own_rows = lax.dynamic_slice_in_dim(silu_pair, lax.axis_index(SP) * rows_block, rows_block, 1)
    partial_mod = jnp.einsum("cd,rde->cre", own_rows, modulation, preferred_element_type=F32)
    partial_mod = partial_mod.reshape(-1, partial_mod.shape[-1])[:5]
    return jnp.sum(from_everyone(partial_mod, SP), axis=0)


def rope_tables(rows_own, width, offsets):
    z_size = lax.axis_size("z")
    lane = jnp.arange(width)
    eighth = width // 8
    inverse = ROPE_BASE ** (-(lane % eighth).astype(F32) / eighth)
    row = lax.axis_index(SP) * z_size + (lax.axis_index("z") + offsets) % z_size
    col = lax.axis_index("core") * rows_own + jnp.arange(rows_own)
    angles = jnp.concatenate([row, col]).astype(F32)[:, None] * inverse
    by_row = (lane % (width // 2)) < width // 4

    def spread(table):
        full = jnp.where(by_row, table[:z_size, None, :], table[None, z_size:, :])
        return full.reshape(z_size * rows_own, width)

    return spread(jnp.cos(angles)), spread(jnp.sin(angles))


def swap_matrix(width):
    source = jnp.arange(width)[:, None]
    target = jnp.arange(width)[None, :]
    eighth = width // 8
    low = target % (2 * eighth) < eighth
    minus = (source == target + eighth) & low
    plus = (source == target - eighth) & ~low
    return plus.astype(BF16) - minus.astype(BF16)


def project(pieces, context, place, vectors, weights, cosine, sine, swap):
    model = vectors.shape[1]
    width = weights[0].shape[1]
    piece_rows = pieces[0].shape[0]
    rows = piece_rows * len(pieces)
    share = context.shape[0] // 2
    total = rows + share
    count = len(pieces)
    step = 16

    def kernel(*refs):
        place_ref, vec, cos_ref, sin_ref, swap_ref = refs[:5]
        token_refs = refs[5 : 5 + count]
        context_ref = refs[5 + count]
        weight_refs = refs[6 + count : 12 + count]
        q_own, kv_own, q_far, kv_far = refs[12 + count : 16 + count]
        tokens, buffer, normed, raw, sems = refs[16 + count :]
        for j in (3, 4, 5, 0, 1, 2):
            pltpu.make_async_copy(weight_refs[j], buffer.at[j], sems.at[j]).start()
        for i, ref in enumerate(token_refs):
            slot = pl.multiple_of(place_ref[i + 1] * piece_rows, piece_rows)
            tokens[pl.ds(slot, piece_rows), :] = ref[...]
        low = pl.multiple_of(place_ref[0] * share, share)
        tokens[rows:, :] = context_ref[pl.ds(low, share), :]

        def normalize(start, base):
            values = tokens[pl.ds(start, step), :].astype(F32)
            center = jnp.mean(values, axis=-1, keepdims=True)
            shifted = values - center
            spread = jnp.mean(shifted * shifted, axis=-1, keepdims=True)
            out = shifted * lax.rsqrt(spread + EPSILON)
            out = out * (1.0 + vec[base + 1 : base + 2, :]) + vec[base : base + 1, :]
            normed[pl.ds(start, step), :] = out.astype(BF16)

        def one_step(i, carry):
            normalize(pl.multiple_of(i * step, step), 0)
            return carry

        lax.fori_loop(0, rows // step, one_step, 0, unroll=UNROLL)
        for low in range(rows, total, step):
            normalize(low, 3)

        def one(i, carry):
            j = lax.rem(i + 3, 6)
            pltpu.make_async_copy(weight_refs[0], buffer.at[j], sems.at[j]).wait()
            product = jnp.dot(normed[...], buffer[j], preferred_element_type=F32)
            raw[j] = product.astype(BF16)

            @pl.when(lax.rem(j, 3) < 2)
            def _():
                value = raw[j, :rows, :]
                turned = jnp.dot(value, swap_ref[...], preferred_element_type=F32)
                value = value.astype(F32) * cos_ref[...] + turned * sin_ref[...]
                raw[j, :rows, :] = value.astype(BF16)

            return carry

        lax.fori_loop(0, 6, one, 0)
        for base, q_ref, kv_ref in ((0, q_own, kv_own), (3, q_far, kv_far)):
            q_ref[...] = raw[base, :rows, :]
            kv_ref[0] = raw[base + 1]
            kv_ref[1] = raw[base + 2]

    vmem = pl.BlockSpec(memory_space=pltpu.VMEM)
    shapes = [(rows, width), (2, total, width)] * 2
    return pl.pallas_call(
        kernel,
        out_shape=[jax.ShapeDtypeStruct(shape, BF16) for shape in shapes],
        in_specs=[pl.BlockSpec(memory_space=pltpu.SMEM)] + [vmem] * (count + 5)
        + [pl.BlockSpec(memory_space=pltpu.HBM)] * 6,
        out_specs=[vmem] * 4,
        scratch_shapes=[
            pltpu.VMEM((total, model), BF16),
            pltpu.VMEM((6, model, width), BF16),
            pltpu.VMEM((total, model), BF16),
            pltpu.VMEM((6, total, width), BF16),
            pltpu.SemaphoreType.DMA((6,)),
        ],
        cost_estimate=pl.CostEstimate(
            flops=2 * 6 * total * model * width, bytes_accessed=12 * model * width, transcendentals=0
        ),
        name="project",
    )(place, vectors, cosine, sine, swap, *pieces, context, *weights)


def join(pairs):
    def kernel(*refs):
        number = 2 * len(pairs)
        for i, ref in enumerate(refs[:number]):
            refs[number + i // 2][i % 2] = ref[...]

    vmem = pl.BlockSpec(memory_space=pltpu.VMEM)
    return pl.pallas_call(
        kernel,
        out_shape=[jax.ShapeDtypeStruct((2, *first.shape), first.dtype) for first, _ in pairs],
        in_specs=[vmem] * (2 * len(pairs)),
        out_specs=[vmem] * len(pairs),
        name="join",
    )(*(array for pair in pairs for array in pair))


def attend(queries, arrays, lift, state=None, final=None, payload=False):
    _, rows, width = queries.shape
    half = width // 2
    number = 2 * len(arrays)
    total = arrays[0].shape[-2]
    scale = half ** (-0.5) * LOG2E
    first, last = state is None, final is not None
    others = final[2] if last else ()
    group = 2

    def kernel(*refs):
        lift_ref, q_ref = refs[:2]
        key_refs = [ref.at[i] for ref in refs[2 : 2 + len(arrays)] for i in range(2)]
        rest = refs[2 + len(arrays) :]
        if not first:
            m_in, l_in, o_in = rest[:3]
            rest = rest[3:]
        if last:
            lambda_ref, gain_ref = rest[:2]
            other_refs = rest[2 : 2 + len(others)]
            out_mine, out_core, out_chip, out_both, scores, accs = rest[2 + len(others) :]
        elif payload:
            out_ref, scores, accs = rest
        else:
            m_out, l_out, o_out, scores, accs = rest
        lift_two = lift_ref[0] * LOG2E
        lanes = lax.broadcasted_iota(jnp.int32, (rows, 128), 1)

        tops, lifteds = [], []
        for m in range(2):
            at = slice(m * half, (m + 1) * half)
            q = q_ref[0, :, at]
            peak = None
            for u, ref in enumerate(key_refs):
                keys = ref[0, :rows, at]
                block = lax.dot_general(q, keys, (((1,), (1,)), ((), ())), preferred_element_type=F32)
                scores[m, :, u * rows : (u + 1) * rows] = block
                for lane in range(0, rows, 128):
                    piece = block[:, lane : lane + 128]
                    peak = piece if peak is None else jnp.maximum(peak, piece)
            keys = jnp.concatenate([ref[0, rows:total, at] for ref in key_refs], axis=0)
            lifted = lax.dot_general(q, keys, (((1,), (1,)), ((), ())), preferred_element_type=F32)
            lifted = lifted * scale + lift_two
            top = jnp.max(peak, axis=1, keepdims=True) * scale
            tops.append(jnp.maximum(top, jnp.max(lifted, axis=1, keepdims=True)))
            lifteds.append(lifted)
        plane = jnp.zeros((rows, 128), F32)
        for m in range(2):
            new, lifted = tops[m], lifteds[m]
            if first:
                total_sum = None
                before = None
            else:
                old = m_in[m, 0, :, :1]
                new = jnp.maximum(old, new)
                fading = jnp.exp2(old - new)
                total_sum = l_in[m, 0] * fading
                before = o_in[m, 0] * fading
            values = jnp.concatenate([ref[1, rows:total, :] for ref in key_refs], axis=0)
            weights = jnp.exp2(lifted - new)
            extra = jnp.sum(weights, axis=1, keepdims=True)
            product = jnp.dot(weights.astype(BF16), values, preferred_element_type=F32)
            accs[m] = product if before is None else before + product
            for u in range(0, number, group):
                weights = jnp.exp2(scores[m, :, u * rows : (u + group) * rows] * scale - new)
                for lane in range(0, group * rows, 128):
                    piece = weights[:, lane : lane + 128]
                    total_sum = piece if total_sum is None else total_sum + piece
                values = jnp.concatenate([ref[1, :rows, :] for ref in key_refs[u : u + group]], axis=0)
                accs[m] += jnp.dot(weights.astype(BF16), values, preferred_element_type=F32)
            if not last and not payload:
                l_out[m, 0] = total_sum + jnp.where(lanes == 0, extra, 0.0)
                m_out[m, 0] = jnp.broadcast_to(new, total_sum.shape)
                o_out[m, 0] = accs[m]
                continue
            row_sums = jnp.sum(total_sum, axis=1, keepdims=True) + extra
            out = accs[m] * (1.0 / row_sums)
            log_sum = new + jnp.log(row_sums) * LOG2E
            if payload:
                out_ref[2 * m, 0] = out[:, :128].astype(BF16)
                out_ref[2 * m + 1, 0] = out[:, 128:].astype(BF16)
                left_over = log_sum
                for k in range(3):
                    piece = left_over.astype(BF16).astype(F32)
                    plane = jnp.where(lanes == 3 * m + k, piece, plane)
                    left_over = left_over - piece
                continue
            source = lax.broadcasted_iota(jnp.int32, (128, 128), 0)
            spread = (source // 3 == m).astype(BF16)
            sizes = [jnp.broadcast_to(log_sum, (rows, 128))]
            sizes += [jnp.dot(ref[4, 0], spread, preferred_element_type=F32) for ref in other_refs]
            top = functools.reduce(jnp.maximum, sizes)
            shares = [jnp.exp2(size - top) for size in sizes]
            inverse = 1.0 / functools.reduce(jnp.add, shares)
            for k in range(2):
                merged = shares[0] * out[:, k * 128 : (k + 1) * 128]
                for share, ref in zip(shares[1:], other_refs):
                    merged = merged + share * ref[2 * m + k, 0].astype(F32)
                accs[m, :, k * 128 : (k + 1) * 128] = merged * inverse
        if payload:
            out_ref[4, 0] = plane.astype(BF16)
        if last:
            difference = accs[0] - lambda_ref[0] * accs[1]
            power = jnp.mean(difference * difference, axis=1, keepdims=True)
            head = (difference * lax.rsqrt(power + EPSILON) * gain_ref[...]).astype(BF16)

            @pl.when(pl.program_id(0) == 0)
            def _():
                out_mine[...] = head[: rows // 2]
                out_chip[...] = head[rows // 2 :]

            @pl.when(pl.program_id(0) == 1)
            def _():
                out_core[...] = head[: rows // 2]
                out_both[...] = head[rows // 2 :]

    smem = pl.BlockSpec(memory_space=pltpu.SMEM)

    def whole(array):
        return pl.BlockSpec(array.shape, lambda i, dims=array.ndim: (0,) * dims)

    narrow = pl.BlockSpec((2, 1, rows, 128), lambda i: (0, i, 0, 0))
    wide = pl.BlockSpec((2, 1, rows, width), lambda i: (0, i, 0, 0))
    planes = pl.BlockSpec((5, 1, rows, 128), lambda i: (0, i, 0, 0))
    inputs = [lift, queries, *arrays]
    by_query = pl.BlockSpec((1, rows, width), lambda i: (i, 0, 0))
    in_specs = [smem, by_query, *(whole(array) for array in arrays)]
    if not first:
        inputs += list(state)
        in_specs += [narrow, narrow, wide]
    if last:
        lambdas, gain, _ = final
        inputs += [lambdas, gain, *others]
        in_specs += [smem, whole(gain), *([planes] * len(others))]
        out_shape = [jax.ShapeDtypeStruct((rows // 2, width), BF16)] * 4
        out_specs = [pl.BlockSpec((rows // 2, width), lambda i: (0, 0))] * 4
    elif payload:
        out_shape = jax.ShapeDtypeStruct((5, 2, rows, 128), BF16)
        out_specs = planes
    else:
        out_shape = [
            jax.ShapeDtypeStruct((2, 2, rows, 128), F32),
            jax.ShapeDtypeStruct((2, 2, rows, 128), F32),
            jax.ShapeDtypeStruct((2, 2, rows, width), F32),
        ]
        out_specs = [narrow, narrow, wide]
    return pl.pallas_call(
        kernel,
        grid=(2,),
        out_shape=out_shape,
        in_specs=in_specs,
        out_specs=out_specs,
        scratch_shapes=[
            pltpu.VMEM((2, rows, number * rows), F32),
            pltpu.VMEM((2, rows, width), F32),
        ],
        cost_estimate=pl.CostEstimate(
            flops=2 * 12 * rows * number * total * half,
            bytes_accessed=4 * number * total * width,
            transcendentals=4 * rows * number * total,
        ),
        name="attend",
    )(*inputs)


def output_product(heads, weights):
    rows, width = heads[0].shape
    model = weights[0].shape[1]
    parts = 4
    part = rows // parts
    number = len(heads)

    def kernel(*refs):
        outs = refs[2 * number :]

        def one(i, carry):
            place = pl.ds(pl.multiple_of(i * OUT_BLOCK, OUT_BLOCK), OUT_BLOCK)
            product = None
            for j in range(number):
                term = jnp.dot(refs[j][...], refs[number + j][:, place], preferred_element_type=F32)
                product = term if product is None else product + term
            for k in range(parts):
                outs[k][:, place] = product[k * part : (k + 1) * part].astype(BF16)
            return carry

        lax.fori_loop(0, model // OUT_BLOCK, one, 0, unroll=OUT_UNROLL)

    vmem = pl.BlockSpec(memory_space=pltpu.VMEM)
    return pl.pallas_call(
        kernel,
        out_shape=[jax.ShapeDtypeStruct((part, model), BF16)] * parts,
        in_specs=[vmem] * (2 * number),
        out_specs=[vmem] * parts,
        cost_estimate=pl.CostEstimate(
            flops=2 * number * rows * width * model,
            bytes_accessed=2 * number * width * model,
            transcendentals=0,
        ),
        name="output_product",
    )(*heads, *weights)


def hop_by_parity(value, axis, step_even, step_odd):
    size = lax.axis_size(axis)
    return lax.ppermute(
        value, axis, [(i, (i + (step_odd if i % 2 else step_even)) % size) for i in range(size)]
    )


def plus(first, second):
    return (first.astype(F32) + second.astype(F32)).astype(BF16)


def steps(
    latent,
    context,
    condition,
    context_condition,
    modulation,
    query_weight,
    key_weight,
    value_weight,
    lambdas,
    context_lift,
    head_gain,
    output_weight,
):
    core = lax.axis_index("core")
    odd = lax.axis_index("z") % 2
    up1, down1 = hop(latent, "z", 1), hop(latent, "z", -1)
    up2 = hop(latent, "z", 2)
    down2 = hop(latent, "z", -2)
    columns = modulation_columns(condition, context_condition, modulation)
    gathered = from_everyone(columns, TP)
    vectors = jnp.moveaxis(gathered, 0, 1).reshape(5, -1)
    up3, down3 = hop(up2, "z", 1), hop(down2, "z", -1)
    opposite = turn_by_core(jnp.where(core == 0, up2, down2), "z", 2)
    pieces = [latent, up1, up2, up3, down1, down2, down3, opposite]
    sign = 2 * odd - 1
    blocks = jnp.arange(8)
    offsets = jnp.where(blocks < 4, sign * blocks, sign * (3 - blocks))
    place = jnp.concatenate(
        [core[None], jnp.array([0, 1, 2, 3, 4, 5, 6, 7]) + jnp.array([0, 3, 3, 3, -3, -3, -3, 0]) * odd]
    ).astype(jnp.int32)

    own_weights = [query_weight, key_weight, value_weight]
    far_weights = [hop(weight, "core", 1) for weight in own_weights]
    core_output = hop(output_weight, "core", 1)
    cosine, sine = rope_tables(latent.shape[0], query_weight.shape[1], offsets)
    swap = swap_matrix(query_weight.shape[1])

    q_a, kv_a, q_send, kv_send = project(
        pieces, context, place, vectors, own_weights + far_weights, cosine, sine, swap
    )
    kv_b = hop(kv_send, "core", 1)
    q_b = hop(q_send, "core", 1)
    later, q_a = lax.optimization_barrier((output_weight, q_a))
    chip_output = hop_by_parity(later, "z", 1, -1)

    def across(value, step):
        return hop_by_core(value, ("x", "y"), step)

    def along(value, step):
        return hop_by_core(value, ("y", "x"), step)

    kv, queries = join([(kv_a, kv_b), (q_a, q_b)])
    kv_p, kv_m = along(kv, 1), along(kv, -1)
    q_p, q_m = across(queries, 1), across(queries, -1)
    kv_on, q_on = lax.optimization_barrier((kv_p, q_m))
    kv_2 = along(kv_on, 1)
    q_2 = across(q_on, -1)

    near = [kv, kv_p, kv_m]
    state = attend(q_m, near, context_lift)
    from_2 = across(attend(q_2, near + [kv_2], context_lift, payload=True), 2)
    from_m = across(attend(q_p, near + [kv_2], context_lift, payload=True), -1)
    ahead = attend(q_m, [kv_2], context_lift, state, payload=True)
    from_p = across(ahead, 1)
    state = attend(queries, near, context_lift)
    mine, for_core, for_chip, for_both = attend(
        queries, [kv_2], context_lift, state, (lambdas, head_gain[None], (from_2, from_m, from_p))
    )

    later, mine = lax.optimization_barrier((chip_output, mine))
    both_output = hop(later, "core", 1)
    of_both = hop(hop_by_parity(for_both, "z", 1, -1), "core", 1)
    of_chip = hop_by_parity(for_chip, "z", 1, -1)
    of_core = hop(for_core, "core", 1)
    share = output_product(
        [mine, of_core, of_chip, of_both], [output_weight, core_output, chip_output, both_output]
    )
    third = hop_by_parity(share[3], "z", -2, 2)
    second = hop_by_parity(share[2], "z", -2, 2)
    first = hop_by_parity(plus(share[1], third), "z", -1, 1)
    mixture = share[0].astype(F32) + second.astype(F32) + first.astype(F32)
    return (latent.astype(F32) + vectors[2] * mixture).astype(BF16)


def solution(mesh):
    split = Mesh(mesh.devices.reshape(4, 4, mesh.shape["tp"] // 2, 2), ALL)
    return jax.shard_map(
        steps,
        mesh=split,
        in_specs=(
            P(ALL, None),
            P(SP, None),
            P(),
            P(),
            P(None, SP, TP),
            P(None, TP),
            P(None, TP),
            P(None, TP),
            P(TP),
            P(TP),
            P(),
            P(TP, None),
        ),
        out_specs=P(ALL, None),
        check_vma=False,
    )
```

```python
import functools
import itertools
import math

import jax
import jax.numpy as jnp
from jax import lax
from jax.experimental import pallas as pl
from jax.experimental.pallas import tpu as pltpu
from jax.sharding import Mesh
from jax.sharding import PartitionSpec as P

ROPE_BASE = 10000.0
EPSILON = 1e-05
LOG2E = math.log2(math.e)
SP = ("y", "x")
TP = ("z", "core")
ALL = SP + TP
F32 = jnp.float32
BF16 = jnp.bfloat16
UNROLL = 2
OUT_BLOCK = 1024
OUT_UNROLL = 1


def hop(value, axis, step):
    size = lax.axis_size(axis)
    return lax.ppermute(value, axis, [(i, (i + step) % size) for i in range(size)])


def hop_by_core(value, axes, step):
    names = tuple(name for name in ALL if name in (*axes, "core"))
    sizes = [lax.axis_size(name) for name in names]
    pairs = []
    for place in itertools.product(*(range(size) for size in sizes)):
        target = list(place)
        at = names.index(axes[place[names.index("core")]])
        target[at] = (target[at] + step) % sizes[at]
        flat = [0, 0]
        for k, where in enumerate((place, target)):
            for size, index in zip(sizes, where):
                flat[k] = flat[k] * size + index
        pairs.append(tuple(flat))
    return lax.ppermute(value, names, pairs)


def turn_by_core(value, axis, step):
    size = lax.axis_size(axis)
    pairs = [
        (2 * i + core, 2 * ((i + (1 - 2 * core) * step) % size) + core) for i in range(size) for core in range(2)
    ]
    return lax.ppermute(value, (axis, "core"), pairs)


def from_everyone(shard, axis):
    copies = jnp.broadcast_to(shard, (lax.axis_size(axis), *shard.shape))
    return lax.all_to_all(copies, axis, split_axis=0, concat_axis=0, tiled=True)


def modulation_columns(condition, context_condition, modulation):
    rows_block = modulation.shape[1]
    silu_pair = jax.nn.silu(jnp.stack([condition, context_condition])).astype(BF16)
    own_rows = lax.dynamic_slice_in_dim(silu_pair, lax.axis_index(SP) * rows_block, rows_block, 1)
    partial_mod = jnp.einsum("cd,rde->cre", own_rows, modulation, preferred_element_type=F32)
    partial_mod = partial_mod.reshape(-1, partial_mod.shape[-1])[:5]
    return jnp.sum(from_everyone(partial_mod, SP), axis=0)


def rope_tables(rows_own, width, offsets):
    z_size = lax.axis_size("z")
    lane = jnp.arange(width)
    eighth = width // 8
    inverse = ROPE_BASE ** (-(lane % eighth).astype(F32) / eighth)
    row = lax.axis_index(SP) * z_size + (lax.axis_index("z") + offsets) % z_size
    col = lax.axis_index("core") * rows_own + jnp.arange(rows_own)
    angles = jnp.concatenate([row, col]).astype(F32)[:, None] * inverse
    by_row = (lane % (width // 2)) < width // 4

    def spread(table):
        full = jnp.where(by_row, table[:z_size, None, :], table[None, z_size:, :])
        return full.reshape(z_size * rows_own, width)

    return spread(jnp.cos(angles)), spread(jnp.sin(angles))


def swap_matrix(width):
    source = jnp.arange(width)[:, None]
    target = jnp.arange(width)[None, :]
    eighth = width // 8
    low = target % (2 * eighth) < eighth
    minus = (source == target + eighth) & low
    plus = (source == target - eighth) & ~low
    return plus.astype(BF16) - minus.astype(BF16)


def project(pieces, context, place, vectors, weights, cosine, sine, swap):
    model = vectors.shape[1]
    width = weights[0].shape[1]
    piece_rows = pieces[0].shape[0]
    rows = piece_rows * len(pieces)
    share = context.shape[0] // 2
    total = rows + share
    count = len(pieces)
    step = 16

    def kernel(*refs):
        place_ref, vec, cos_ref, sin_ref, swap_ref = refs[:5]
        token_refs = refs[5 : 5 + count]
        context_ref = refs[5 + count]
        weight_refs = refs[6 + count : 12 + count]
        q_own, kv_own, q_far, kv_far = refs[12 + count : 16 + count]
        tokens, buffer, normed, raw, sems = refs[16 + count :]
        for j in (3, 4, 5, 0, 1, 2):
            pltpu.make_async_copy(weight_refs[j], buffer.at[j], sems.at[j]).start()
        for i, ref in enumerate(token_refs):
            slot = pl.multiple_of(place_ref[i + 1] * piece_rows, piece_rows)
            tokens[pl.ds(slot, piece_rows), :] = ref[...]
        low = pl.multiple_of(place_ref[0] * share, share)
        tokens[rows:, :] = context_ref[pl.ds(low, share), :]

        def normalize(start, base):
            values = tokens[pl.ds(start, step), :].astype(F32)
            center = jnp.mean(values, axis=-1, keepdims=True)
            shifted = values - center
            spread = jnp.mean(shifted * shifted, axis=-1, keepdims=True)
            out = shifted * lax.rsqrt(spread + EPSILON)
            out = out * (1.0 + vec[base + 1 : base + 2, :]) + vec[base : base + 1, :]
            normed[pl.ds(start, step), :] = out.astype(BF16)

        def one_step(i, carry):
            normalize(pl.multiple_of(i * step, step), 0)
            return carry

        lax.fori_loop(0, rows // step, one_step, 0, unroll=UNROLL)
        for low in range(rows, total, step):
            normalize(low, 3)

        def one(i, carry):
            j = lax.rem(i + 3, 6)
            pltpu.make_async_copy(weight_refs[0], buffer.at[j], sems.at[j]).wait()
            product = jnp.dot(normed[...], buffer[j], preferred_element_type=F32)
            raw[j] = product.astype(BF16)

            @pl.when(lax.rem(j, 3) < 2)
            def _():
                value = raw[j, :rows, :]
                turned = jnp.dot(value, swap_ref[...], preferred_element_type=F32)
                value = value.astype(F32) * cos_ref[...] + turned * sin_ref[...]
                raw[j, :rows, :] = value.astype(BF16)

            return carry

        lax.fori_loop(0, 6, one, 0)
        for base, q_ref, kv_ref in ((0, q_own, kv_own), (3, q_far, kv_far)):
            q_ref[...] = raw[base, :rows, :]
            kv_ref[0] = raw[base + 1]
            kv_ref[1] = raw[base + 2]

    vmem = pl.BlockSpec(memory_space=pltpu.VMEM)
    shapes = [(rows, width), (2, total, width)] * 2
    return pl.pallas_call(
        kernel,
        out_shape=[jax.ShapeDtypeStruct(shape, BF16) for shape in shapes],
        in_specs=[pl.BlockSpec(memory_space=pltpu.SMEM)] + [vmem] * (count + 5)
        + [pl.BlockSpec(memory_space=pltpu.HBM)] * 6,
        out_specs=[vmem] * 4,
        scratch_shapes=[
            pltpu.VMEM((total, model), BF16),
            pltpu.VMEM((6, model, width), BF16),
            pltpu.VMEM((total, model), BF16),
            pltpu.VMEM((6, total, width), BF16),
            pltpu.SemaphoreType.DMA((6,)),
        ],
        cost_estimate=pl.CostEstimate(
            flops=2 * 6 * total * model * width, bytes_accessed=12 * model * width, transcendentals=0
        ),
        compiler_params=pltpu.CompilerParams(vmem_limit_bytes=48 * 2**20),
        name="project",
    )(place, vectors, cosine, sine, swap, *pieces, context, *weights)


def join(pairs):
    def kernel(*refs):
        number = 2 * len(pairs)
        for i, ref in enumerate(refs[:number]):
            refs[number + i // 2][i % 2] = ref[...]

    vmem = pl.BlockSpec(memory_space=pltpu.VMEM)
    return pl.pallas_call(
        kernel,
        out_shape=[jax.ShapeDtypeStruct((2, *first.shape), first.dtype) for first, _ in pairs],
        in_specs=[vmem] * (2 * len(pairs)),
        out_specs=[vmem] * len(pairs),
        compiler_params=pltpu.CompilerParams(vmem_limit_bytes=6 * 2**20),
        name="join",
    )(*(array for pair in pairs for array in pair))


def attend(queries, arrays, lift, state=None, final=None, payload=False):
    _, rows, width = queries.shape
    half = width // 2
    number = 2 * len(arrays)
    total = arrays[0].shape[-2]
    scale = half ** (-0.5) * LOG2E
    first, last = state is None, final is not None
    others = final[2] if last else ()
    group = 2

    def kernel(*refs):
        lift_ref, q_ref = refs[:2]
        key_refs = [ref.at[i] for ref in refs[2 : 2 + len(arrays)] for i in range(2)]
        rest = refs[2 + len(arrays) :]
        if not first:
            m_in, l_in, o_in = rest[:3]
            rest = rest[3:]
        if last:
            lambda_ref, gain_ref = rest[:2]
            other_refs = rest[2 : 2 + len(others)]
            out_mine, out_core, out_chip, out_both, scores, accs = rest[2 + len(others) :]
        elif payload:
            out_ref, scores, accs = rest
        else:
            m_out, l_out, o_out, scores, accs = rest
        lift_two = lift_ref[0] * LOG2E

        def one_block(block, carry):
            lanes = lax.broadcasted_iota(jnp.int32, (rows, 128), 1)

            tops, lifteds = [], []
            for m in range(2):
                at = slice(m * half, (m + 1) * half)
                q = q_ref[block, :, at]
                peak = None
                for u, ref in enumerate(key_refs):
                    keys = ref[0, :rows, at]
                    products = lax.dot_general(q, keys, (((1,), (1,)), ((), ())), preferred_element_type=F32)
                    scores[m, :, u * rows : (u + 1) * rows] = products
                    for lane in range(0, rows, 128):
                        piece = products[:, lane : lane + 128]
                        peak = piece if peak is None else jnp.maximum(peak, piece)
                keys = jnp.concatenate([ref[0, rows:total, at] for ref in key_refs], axis=0)
                lifted = lax.dot_general(q, keys, (((1,), (1,)), ((), ())), preferred_element_type=F32)
                lifted = lifted * scale + lift_two
                top = jnp.max(peak, axis=1, keepdims=True) * scale
                tops.append(jnp.maximum(top, jnp.max(lifted, axis=1, keepdims=True)))
                lifteds.append(lifted)
            plane = jnp.zeros((rows, 128), F32)
            for m in range(2):
                new, lifted = tops[m], lifteds[m]
                if first:
                    total_sum = None
                    before = None
                else:
                    old = m_in[m, block, :, :1]
                    new = jnp.maximum(old, new)
                    fading = jnp.exp2(old - new)
                    total_sum = l_in[m, block] * fading
                    before = o_in[m, block] * fading
                values = jnp.concatenate([ref[1, rows:total, :] for ref in key_refs], axis=0)
                weights = jnp.exp2(lifted - new)
                extra = jnp.sum(weights, axis=1, keepdims=True)
                product = jnp.dot(weights.astype(BF16), values, preferred_element_type=F32)
                accs[m] = product if before is None else before + product
                for u in range(0, number, group):
                    weights = jnp.exp2(scores[m, :, u * rows : (u + group) * rows] * scale - new)
                    for lane in range(0, group * rows, 128):
                        piece = weights[:, lane : lane + 128]
                        total_sum = piece if total_sum is None else total_sum + piece
                    values = jnp.concatenate([ref[1, :rows, :] for ref in key_refs[u : u + group]], axis=0)
                    accs[m] += jnp.dot(weights.astype(BF16), values, preferred_element_type=F32)
                if not last and not payload:
                    l_out[m, block] = total_sum + jnp.where(lanes == 0, extra, 0.0)
                    m_out[m, block] = jnp.broadcast_to(new, total_sum.shape)
                    o_out[m, block] = accs[m]
                    continue
                row_sums = jnp.sum(total_sum, axis=1, keepdims=True) + extra
                out = accs[m] * (1.0 / row_sums)
                log_sum = new + jnp.log(row_sums) * LOG2E
                if payload:
                    out_ref[2 * m, block] = out[:, :128].astype(BF16)
                    out_ref[2 * m + 1, block] = out[:, 128:].astype(BF16)
                    left_over = log_sum
                    for k in range(3):
                        piece = left_over.astype(BF16).astype(F32)
                        plane = jnp.where(lanes == 3 * m + k, piece, plane)
                        left_over = left_over - piece
                    continue
                source = lax.broadcasted_iota(jnp.int32, (128, 128), 0)
                spread = (source // 3 == m).astype(BF16)
                sizes = [jnp.broadcast_to(log_sum, (rows, 128))]
                sizes += [jnp.dot(ref[4, block], spread, preferred_element_type=F32) for ref in other_refs]
                top = functools.reduce(jnp.maximum, sizes)
                shares = [jnp.exp2(size - top) for size in sizes]
                inverse = 1.0 / functools.reduce(jnp.add, shares)
                for k in range(2):
                    merged = shares[0] * out[:, k * 128 : (k + 1) * 128]
                    for share, ref in zip(shares[1:], other_refs):
                        merged = merged + share * ref[2 * m + k, block].astype(F32)
                    accs[m, :, k * 128 : (k + 1) * 128] = merged * inverse
            if payload:
                out_ref[4, block] = plane.astype(BF16)
            if last:
                difference = accs[0] - lambda_ref[0] * accs[1]
                power = jnp.mean(difference * difference, axis=1, keepdims=True)
                head = (difference * lax.rsqrt(power + EPSILON) * gain_ref[...]).astype(BF16)

                @pl.when(block == 0)
                def _():
                    out_mine[...] = head[: rows // 2]
                    out_chip[...] = head[rows // 2 :]

                @pl.when(block == 1)
                def _():
                    out_core[...] = head[: rows // 2]
                    out_both[...] = head[rows // 2 :]
            return carry

        lax.fori_loop(0, 2, one_block, 0)

    smem = pl.BlockSpec(memory_space=pltpu.SMEM)
    vmem = pl.BlockSpec(memory_space=pltpu.VMEM)
    inputs = [lift, queries, *arrays]
    in_specs = [smem, vmem, *([vmem] * len(arrays))]
    if not first:
        inputs += list(state)
        in_specs += [vmem] * 3
    if last:
        lambdas, gain, _ = final
        inputs += [lambdas, gain, *others]
        in_specs += [smem, vmem, *([vmem] * len(others))]
        out_shape = [jax.ShapeDtypeStruct((rows // 2, width), BF16)] * 4
        out_specs = [vmem] * 4
    elif payload:
        out_shape = jax.ShapeDtypeStruct((5, 2, rows, 128), BF16)
        out_specs = vmem
    else:
        out_shape = [
            jax.ShapeDtypeStruct((2, 2, rows, 128), F32),
            jax.ShapeDtypeStruct((2, 2, rows, 128), F32),
            jax.ShapeDtypeStruct((2, 2, rows, width), F32),
        ]
        out_specs = [vmem] * 3
    return pl.pallas_call(
        kernel,
        out_shape=out_shape,
        in_specs=in_specs,
        out_specs=out_specs,
        scratch_shapes=[
            pltpu.VMEM((2, rows, number * rows), F32),
            pltpu.VMEM((2, rows, width), F32),
        ],
        cost_estimate=pl.CostEstimate(
            flops=2 * 12 * rows * number * total * half,
            bytes_accessed=4 * number * total * width,
            transcendentals=4 * rows * number * total,
        ),
        compiler_params=pltpu.CompilerParams(vmem_limit_bytes=16 * 2**20),
        name="attend",
    )(*inputs)


def output_product(heads, weights):
    rows, width = heads[0].shape
    model = weights[0].shape[1]
    parts = 4
    part = rows // parts
    number = len(heads)

    def kernel(*refs):
        outs, (buffer, sems) = refs[2 * number : -2], refs[-2:]

        def copy(i, j):
            place = pl.ds(pl.multiple_of(i * OUT_BLOCK, OUT_BLOCK), OUT_BLOCK)
            return pltpu.make_async_copy(refs[number + j].at[:, place], buffer.at[i, j], sems.at[i, j])

        for i in range(model // OUT_BLOCK):
            for j in range(number):
                copy(i, j).start()

        def one(i, carry):
            place = pl.ds(pl.multiple_of(i * OUT_BLOCK, OUT_BLOCK), OUT_BLOCK)
            product = None
            for j in range(number):
                copy(i, j).wait()
            for j in range(number):
                term = jnp.dot(refs[j][...], buffer[i, j], preferred_element_type=F32)
                product = term if product is None else product + term
            for k in range(parts):
                outs[k][:, place] = product[k * part : (k + 1) * part].astype(BF16)
            return carry

        lax.fori_loop(0, model // OUT_BLOCK, one, 0, unroll=OUT_UNROLL)

    vmem = pl.BlockSpec(memory_space=pltpu.VMEM)
    return pl.pallas_call(
        kernel,
        out_shape=[jax.ShapeDtypeStruct((part, model), BF16)] * parts,
        in_specs=[vmem] * number + [pl.BlockSpec(memory_space=pltpu.HBM)] * number,
        out_specs=[vmem] * parts,
        scratch_shapes=[
            pltpu.VMEM((model // OUT_BLOCK, number, width, OUT_BLOCK), BF16),
            pltpu.SemaphoreType.DMA((model // OUT_BLOCK, number)),
        ],
        cost_estimate=pl.CostEstimate(
            flops=2 * number * rows * width * model,
            bytes_accessed=2 * number * width * model,
            transcendentals=0,
        ),
        compiler_params=pltpu.CompilerParams(vmem_limit_bytes=16 * 2**20),
        name="output_product",
    )(*heads, *weights)


def hop_by_parity(value, axis, step_even, step_odd):
    size = lax.axis_size(axis)
    return lax.ppermute(
        value, axis, [(i, (i + (step_odd if i % 2 else step_even)) % size) for i in range(size)]
    )


def plus(first, second):
    return (first.astype(F32) + second.astype(F32)).astype(BF16)


def steps(
    latent,
    context,
    condition,
    context_condition,
    modulation,
    query_weight,
    key_weight,
    value_weight,
    lambdas,
    context_lift,
    head_gain,
    output_weight,
):
    core = lax.axis_index("core")
    odd = lax.axis_index("z") % 2
    up2, down2 = hop(latent, "z", 2), hop(latent, "z", -2)
    columns = modulation_columns(condition, context_condition, modulation)
    up1, down1 = hop(latent, "z", 1), hop(latent, "z", -1)
    gathered = from_everyone(columns, TP)
    vectors = jnp.moveaxis(gathered, 0, 1).reshape(5, -1)
    up3, down3 = hop(up2, "z", 1), hop(down2, "z", -1)
    opposite = turn_by_core(jnp.where(core == 0, up2, down2), "z", 2)
    pieces = [latent, up1, up2, up3, down1, down2, down3, opposite]
    sign = 2 * odd - 1
    blocks = jnp.arange(8)
    offsets = jnp.where(blocks < 4, sign * blocks, sign * (3 - blocks))
    place = jnp.concatenate(
        [core[None], jnp.array([0, 1, 2, 3, 4, 5, 6, 7]) + jnp.array([0, 3, 3, 3, -3, -3, -3, 0]) * odd]
    ).astype(jnp.int32)

    own_weights = [query_weight, key_weight, value_weight]
    far_weights = [hop(weight, "core", 1) for weight in own_weights]
    core_output = hop(output_weight, "core", 1)
    cosine, sine = rope_tables(latent.shape[0], query_weight.shape[1], offsets)
    swap = swap_matrix(query_weight.shape[1])

    q_a, kv_a, q_send, kv_send = project(
        pieces, context, place, vectors, own_weights + far_weights, cosine, sine, swap
    )
    kv_b = hop(kv_send, "core", 1)
    q_b = hop(q_send, "core", 1)
    later, q_a = lax.optimization_barrier((output_weight, q_a))
    chip_output = hop_by_parity(later, "z", 1, -1)

    def across(value, step):
        return hop_by_core(value, ("x", "y"), step)

    def along(value, step):
        return hop_by_core(value, ("y", "x"), step)

    kv, queries = join([(kv_a, kv_b), (q_a, q_b)])
    kv_p, kv_m = along(kv, 1), along(kv, -1)
    q_p, q_m = across(queries, 1), across(queries, -1)
    kv_on, q_on = lax.optimization_barrier((kv_p, q_m))
    kv_2 = along(kv_on, 1)
    q_2 = across(q_on, -1)

    near = [kv, kv_p, kv_m]
    state = attend(q_m, near, context_lift)
    from_2 = across(attend(q_2, near + [kv_2], context_lift, payload=True), 2)
    from_m = across(attend(q_p, near + [kv_2], context_lift, payload=True), -1)
    ahead = attend(q_m, [kv_2], context_lift, state, payload=True)
    from_p = across(ahead, 1)
    state = attend(queries, near, context_lift)
    mine, for_core, for_chip, for_both = attend(
        queries, [kv_2], context_lift, state, (lambdas, head_gain[None], (from_2, from_m, from_p))
    )

    later, mine = lax.optimization_barrier((chip_output, mine))
    both_output = hop(later, "core", 1)
    of_both = hop(hop_by_parity(for_both, "z", 1, -1), "core", 1)
    of_chip = hop_by_parity(for_chip, "z", 1, -1)
    of_core = hop(for_core, "core", 1)
    share = output_product(
        [mine, of_core, of_chip, of_both], [output_weight, core_output, chip_output, both_output]
    )
    third = hop_by_parity(share[3], "z", -2, 2)
    second = hop_by_parity(share[2], "z", -2, 2)
    first = hop_by_parity(plus(share[1], third), "z", -1, 1)
    mixture = share[0].astype(F32) + second.astype(F32) + first.astype(F32)
    return (latent.astype(F32) + vectors[2] * mixture).astype(BF16)


def solution(mesh):
    split = Mesh(mesh.devices.reshape(4, 4, mesh.shape["tp"] // 2, 2), ALL)
    return jax.shard_map(
        steps,
        mesh=split,
        in_specs=(
            P(ALL, None),
            P(SP, None),
            P(),
            P(),
            P(None, SP, TP),
            P(None, TP),
            P(None, TP),
            P(None, TP),
            P(TP),
            P(TP),
            P(),
            P(TP, None),
        ),
        out_specs=P(ALL, None),
        check_vma=False,
    )
```
